32 devices in a mesh: grp: 2 (over x), ep: 16 (over z, y, core).
Axes of the slice: x: 2, y: 2, z: 4, core: 2. Of those that a mesh axis runs over, the one named last changes fastest.
Arguments:
- tokens: bfloat16 [4096, 2048], P(('grp', 'ep')), parts along dimension 0, may hold values from -6 to 6
- norm_gain: float32 [2048], replicated, may hold values from 0.1 to 1.9
- expert_ids: int32 [4096, 2], P(('grp', 'ep')), parts along dimension 0, may hold values from 0 to 3, all different within a row; in each aligned block of 128 rows (0 to 127, 128 to 255, ...) at most 128 rows name the same one
- route_weight: float32 [4096, 2], P(('grp', 'ep')), parts along dimension 0, may hold values from 0.1 to 1
- gate_weight: bfloat16 [16, 2048, 512], P('ep'), may hold values from -0.375 to 0.375
- up_weight: bfloat16 [16, 2048, 512], P('ep'), may hold values from -0.375 to 0.375
- down_weight: bfloat16 [16, 512, 2048], P('ep'), may hold values from -0.03125 to 0.03125
Outputs:
- combined: bfloat16 [4096, 2048], P(('grp', 'ep')), parts along dimension 0
The draws below stay inside these ranges and needn't reach their ends.
There are 2 independent parts, one for each index of `grp`. The reference program is written for one: setup_inputs(seed, part) draws one part's arguments, and reference() takes and returns one part's arrays. A program takes and returns all parts, laid end to end along the dimension named above; an argument that names none is the same for every part. Nothing has to cross between parts.
Inputs may be any that keep to these rules, and one draw needn't show every extreme that they name: `expert_ids`: each token names 2 different experts; among the tokens of one device no expert is named more than 128 times, and in every draw some expert is named exactly 128 times by the tokens of some device.
All inputs are finite; a program needn't handle non-finite values.
Results may differ from the reference program's by a relative error of at most 0.0078.
Values may be sent and summed in bfloat16 or wider, within the bound.
A program may use at most 128 MiB of HBM per device.

```python
import math
import jax
import jax.numpy as jnp
import numpy as np
from jax import lax

D = 2048
FF = 2048
SPLIT = 4
FF_DEV = 512
TOP_K = 2
TOK_DEV = 128
EXPERTS = 4
CAP = 128
TOKENS = 2048
N_EP = 16


def levels(stream_key, extent, pieces, low, largest):
    factor_of, own = 1.0, jax.random.fold_in(stream_key, 6)
    for position, shards_of in pieces:
        steps = jnp.exp(jax.random.uniform(jax.random.fold_in(own, position), (shards_of,), jnp.float32, low / len(pieces), largest / len(pieces)))
        factor_of = factor_of * jnp.repeat(steps, extent[position] // shards_of).reshape([-1 if axis == position else 1 for axis in range(len(extent))])
    return factor_of


def assign_block(own_key, own, number, rows, amount, top, bound, skew):
    sequence = jax.random.permutation(own_key, amount)
    crowded, ordinary = shares(amount, rows * top, bound, skew, True), shares(amount, rows * top, bound, skew, False)
    places = jnp.arange(amount)

    def named(tallies, turn):
        used = int((tallies > 0).sum())
        fixed = max(1, used // 4)
        shifted = fixed + (places - fixed + turn * (used - fixed)) % max(1, amount - fixed)
        return jnp.zeros((amount,), jnp.int32).at[sequence[jnp.where(places < fixed, places, shifted)]].set(jnp.asarray(tallies, jnp.int32))

    tallies = jnp.where(number % 4 == 0, named(crowded, number // 4), named(ordinary, number - number // 4 - 1))
    mixed = jax.random.permutation(jax.random.fold_in(own, 3), amount)
    source_of, receiver = mixed[0:amount // 2 * 2:2], mixed[1:amount // 2 * 2:2]
    margin = jnp.minimum(tallies[source_of] - 1, bound - tallies[receiver]) // 2
    margin = jnp.where((source_of == sequence[0]) | (receiver == sequence[0]) | (tallies[receiver] == 0), 0, jnp.maximum(margin, 0))
    shifted = jax.random.randint(jax.random.fold_in(own, 4), (amount // 2,), 0, 1 << 20) % (margin + 1)
    tallies = tallies.at[source_of].add(-shifted).at[receiver].add(shifted)
    items = jnp.searchsorted(jnp.cumsum(tallies), jnp.arange(rows * top), side="right").astype(jnp.int32)
    table = items.reshape(top, rows).T
    table = table[jax.random.permutation(jax.random.fold_in(own, 1), rows)]
    turn = jax.random.randint(jax.random.fold_in(own, 2), (rows, 1), 0, top)
    return jnp.take_along_axis(table, (jnp.arange(top)[None, :] + turn) % top, axis=1)


def shares(amount, total, limit, slope, full):
    loads = [(1 << 20) // math.isqrt(rank ** slope) + 1 for rank in range(1, amount + 1)]
    largest = limit if full else min(limit, max(-(-total // amount), total * loads[0] // sum(loads)))
    least = 1 if total - largest >= amount - 1 else 0
    holding, rest = [largest] + [least] * (amount - 1), total - largest - least * (amount - 1)
    while rest > 0:
        candidates = [i for i in range(1, amount) if holding[i] < largest] or [i for i in range(1, amount) if holding[i] < limit]
        whole, budget = sum([loads[i] for i in candidates]), rest
        for i in candidates:
            extra = min(limit - holding[i], max(1, budget * loads[i] // whole), rest)
            holding[i] = holding[i] + extra
            rest = rest - extra
    return np.array(holding)


def normal_values(stream_key, dims, width, reach, cuts=(), held_as=jnp.bfloat16):
    drawn = width * jax.random.normal(stream_key, dims, jnp.float32)
    if cuts:
        drawn = drawn * levels(stream_key, dims, cuts, -0.22, 0.18)
    return jnp.clip(drawn, -reach, reach).astype(held_as)


def setup_inputs(seed: int = 0, part: int = 0) -> dict:
    key_list = jax.random.split(jax.random.key(seed), 8)
    part_keys = jax.random.split(jax.random.fold_in(key_list[7], part), 8)
    tokens = normal_values(part_keys[0], (TOKENS, D), 1.0, 6.0, ((0, 16),))
    norm_gain = jnp.clip(1.0 + 0.18 * jax.random.normal(key_list[1], (D,), jnp.float32), 0.1, 1.9)
    expert_ids_keys = jax.random.split(jax.random.fold_in(part_keys[2], 1), TOKENS // TOK_DEV)
    expert_ids_turns = jax.random.permutation(jax.random.fold_in(part_keys[2], 3), TOKENS // TOK_DEV)
    expert_ids = jax.vmap(lambda own, number: assign_block(jax.random.fold_in(part_keys[2], 2), own, number, TOK_DEV, EXPERTS, TOP_K, CAP, 2))(expert_ids_keys, expert_ids_turns).reshape((TOKENS, TOP_K))
    route_weight = jnp.clip(jnp.exp(math.log(1.0) - 2.3025851 * jax.random.uniform(part_keys[3], (TOKENS, TOP_K), jnp.float32) ** levels(part_keys[3], (TOKENS, TOP_K), ((0, 16),), -0.2, 0.2)), 0.1, 1.0)
    gate_weight = normal_values(key_list[4], (N_EP, D, FF_DEV), (D // 8) ** -0.5, 0.375, ((0, 16),))
    up_weight = normal_values(key_list[5], (N_EP, D, FF_DEV), (D // 8) ** -0.5, 0.375, ((0, 16),))
    down_weight = normal_values(key_list[6], (N_EP, FF_DEV, D), (16 * FF) ** -0.5, 0.03125, ((0, 16),))
    return dict(tokens=tokens, norm_gain=norm_gain, expert_ids=expert_ids, route_weight=route_weight, gate_weight=gate_weight, up_weight=up_weight, down_weight=down_weight)


EPSILON = 1e-05
clamp_limit = 7.0
sigmoid_slope = 1.702
row_block = 256

def reference(tokens, norm_gain, expert_ids, route_weight, gate_weight, up_weight, down_weight):
    values = tokens.astype(jnp.float32)
    center = values - lax.optimization_barrier(jnp.mean(values, axis=-1, keepdims=True))
    spread = lax.optimization_barrier(jnp.mean(center * center, axis=-1, keepdims=True))
    normed = (center * lax.rsqrt(spread + EPSILON) * norm_gain).astype(jnp.bfloat16)
    w_gate = gate_weight.reshape(EXPERTS, SPLIT, D, FF_DEV).transpose(0, 2, 1, 3).reshape(EXPERTS, D, FF)
    w_up = up_weight.reshape(EXPERTS, SPLIT, D, FF_DEV).transpose(0, 2, 1, 3).reshape(EXPERTS, D, FF)
    w_down = down_weight.reshape(EXPERTS, FF, D)
    assigned = TOKENS * TOP_K
    flat_ids = expert_ids.reshape(assigned).astype(jnp.int32)
    owners = jnp.arange(assigned, dtype=jnp.int32) // TOP_K
    ranking = jnp.argsort(flat_ids, stable=True).astype(jnp.int32)
    sorted_ids = flat_ids[ranking]
    counts = lax.optimization_barrier(jnp.sum((flat_ids[:, None] == jnp.arange(EXPERTS, dtype=jnp.int32)[None, :]).astype(jnp.int32), axis=0))
    starts = jnp.cumsum(counts) - counts
    padded_counts = (counts + row_block - 1) // row_block * row_block
    block_ends = jnp.cumsum(padded_counts)
    begins = block_ends - padded_counts
    target = (begins[sorted_ids] + jnp.arange(assigned, dtype=jnp.int32) - starts[sorted_ids]).astype(jnp.int32)
    blocks = -(-assigned // row_block) + EXPERTS
    slot_token = jnp.full((blocks * row_block,), TOKENS, jnp.int32).at[target].set(owners[ranking])
    first_rows = jnp.arange(blocks, dtype=jnp.int32) * row_block
    block_expert = jnp.minimum(lax.optimization_barrier(jnp.sum((first_rows[:, None] >= block_ends[None, :]).astype(jnp.int32), axis=1)), EXPERTS - 1).astype(jnp.int32)
    padded = jnp.concatenate([normed, jnp.zeros((1, D), jnp.bfloat16)], axis=0)
    gathered_rows = jnp.take(padded, slot_token, axis=0).reshape(blocks, row_block, D)

    def block_fn(operands):
        block_rows, expert = operands
        gate_pre = jnp.dot(block_rows, w_gate[expert], preferred_element_type=jnp.float32)
        up_pre = jnp.dot(block_rows, w_up[expert], preferred_element_type=jnp.float32)
        gate_cut = jnp.minimum(gate_pre, clamp_limit)
        up_cut = jnp.clip(up_pre, -clamp_limit, clamp_limit)
        active = ((up_cut + 1.0) * (gate_cut * jax.nn.sigmoid(gate_cut * sigmoid_slope))).astype(jnp.bfloat16)
        return jnp.dot(active, w_down[expert], preferred_element_type=jnp.float32).astype(jnp.bfloat16)
    outputs = lax.map(block_fn, (gathered_rows, block_expert)).reshape(blocks * row_block, D)
    sorted_out = jnp.take(outputs, target, axis=0)
    picked = jnp.zeros((assigned, D), jnp.bfloat16).at[ranking].set(sorted_out).reshape(TOKENS, TOP_K, D)
    combined = lax.optimization_barrier(jnp.sum(route_weight[:, :, None] * picked.astype(jnp.float32), axis=1))
    return combined.astype(jnp.bfloat16)
```

```python
import functools

import jax
import jax.numpy as jnp
from jax import lax
from jax.experimental import pallas as pl
from jax.experimental.pallas import tpu as pltpu
from jax.sharding import PartitionSpec as P

SPLIT = 4


EPSILON = 1e-05
clamp_limit = 7.0
sigmoid_slope = 1.702


def swapped(array, axis, bit):
    return lax.ppermute(array, axis, [(i, i ^ 1 << bit) for i in range(lax.axis_size(axis))])


def layer_norm(tokens, norm_gain):
    values = tokens.astype(jnp.float32)
    center = values - jnp.mean(values, axis=-1, keepdims=True)
    spread = jnp.mean(center * center, axis=-1, keepdims=True)
    return (center * lax.rsqrt(spread + EPSILON) * norm_gain).astype(jnp.bfloat16)


def expert_rows(block_rows, gate_weight, up_weight, down_weight):
    gate_pre = jnp.einsum(
        "scd,df->scf", block_rows, gate_weight[0], preferred_element_type=jnp.float32
    )
    up_pre = jnp.einsum("scd,df->scf", block_rows, up_weight[0], preferred_element_type=jnp.float32)
    gate_cut = jnp.minimum(gate_pre, clamp_limit)
    up_cut = jnp.clip(up_pre, -clamp_limit, clamp_limit)
    active = ((up_cut + 1.0) * (gate_cut * jax.nn.sigmoid(gate_cut * sigmoid_slope))).astype(
        jnp.bfloat16
    )
    return jnp.einsum("scf,fd->scd", active, down_weight[0], preferred_element_type=jnp.float32)


def slot_body(tokens, norm_gain, expert_ids, route_weight, gate_weight, up_weight, down_weight):
    normed = layer_norm(tokens, norm_gain)
    devices = lax.axis_size("ep")
    experts = devices // SPLIT
    tok_rows = tokens.shape[0]
    top_count = expert_ids.shape[1]
    width = tokens.shape[1]
    capacity = min(tok_rows, 2 * tok_rows * top_count // experts)
    quarter = capacity // SPLIT
    levels = SPLIT.bit_length() - 1
    position = lax.axis_index("ep")
    flat_ids = expert_ids.reshape(-1)
    onehot = (flat_ids[:, None] == jnp.arange(experts, dtype=jnp.int32)[None, :]).astype(jnp.int32)
    earlier = jnp.cumsum(onehot, axis=0) - onehot
    slot_index = jnp.sum(earlier * onehot, axis=1)
    target = flat_ids * capacity + slot_index
    owners = jnp.arange(flat_ids.shape[0], dtype=jnp.int32) // top_count
    slot_token = jnp.full((experts * capacity,), tok_rows, jnp.int32).at[target].set(owners)
    padded = jnp.concatenate([normed, jnp.zeros((1, width), jnp.bfloat16)], axis=0)
    outgoing = jnp.take(padded, slot_token, axis=0).reshape(experts, capacity, width)
    pieces = outgoing.reshape(devices, quarter, width)
    gathered = lax.all_to_all(pieces, "ep", split_axis=0, concat_axis=0, tiled=True)
    for bit_level in range(levels):
        partner = swapped(gathered, "ep", bit_level)
        upper_bit = position >> bit_level & 1
        first_half = jnp.where(upper_bit == 1, partner, gathered)
        second_half = jnp.where(upper_bit == 1, gathered, partner)
        gathered = jnp.concatenate([first_half, second_half], axis=1)
    partial_value = expert_rows(gathered, gate_weight, up_weight, down_weight)
    length = capacity
    for bit_level in reversed(range(levels)):
        length = length // 2
        upper_bit = position >> bit_level & 1
        kept_rows = lax.dynamic_slice_in_dim(partial_value, upper_bit * length, length, 1)
        sent_rows = lax.dynamic_slice_in_dim(partial_value, (1 - upper_bit) * length, length, 1)
        partial_value = kept_rows + swapped(sent_rows, "ep", bit_level)
    finished = partial_value.astype(jnp.bfloat16)
    returned = lax.all_to_all(finished, "ep", split_axis=0, concat_axis=0, tiled=True)
    results = returned.reshape(experts * capacity, width)
    picked = jnp.take(results, target, axis=0).reshape(tok_rows, top_count, width)
    combined = jnp.sum(route_weight[:, :, None] * picked.astype(jnp.float32), axis=1)
    return combined.astype(jnp.bfloat16)


MESH = pl.DeviceIdType.MESH
PLANES = 4
PIECES = 4

RELAY, CROSS, COMPUTE, SETTLE = 0, 1, 2, 3
GROUP = 8
END_WORDS = (
    32897, 262209, 335609865, 2373642, 13631520, 11534409,
    6341706, 1312779, 557072, 69566664, 6612242, 7340112,
    3408008, 67731480, 170459161, 68517936, 7110872, 2657386,
    69828745, 300744936, 1837163, 5347714, 8126648, 74311474,
    6815864, 201130096, 68780272, 121438267, 75333784, 259063995,
    4032627, 166264920, 5767411, 1149211, 98109851, 5505168,
    5870058, 82413915, 7706002, 80314539, 82150115, 80052835,
    230791939, 228694979,
)
MID_WORDS = (
    6586377, 8388648, 279248897, 557584, 19411242, 14680201,
    6340810, 17563680, 7602592, 11534361, 1573592, 23606306,
    10485969, 300744921, 2654264, 22806912, 20709800, 245965522,
    101297978, 24641609, 5344442, 69042424, 3670680, 7700704,
    103388610, 3408472, 326697648, 21495931, 6131811, 263785691,
    102335011, 108893786, 239927539, 104436419, 111216171, 5868571,
    158438018, 53841307, 112041739, 115970819, 5608323, 113876811,
    266703427, 139147,
)
END_SENT = (12, 6, 0, 32, 32, 28)
END_TILES = (4, 1, 0, 8)
MID_SENT = (11, 11, 16, 32, 32, 28)
MID_TILES = (4, 2, 3, 8)


def lane_column(row, piece, rows):
    lanes = lax.broadcasted_iota(jnp.int32, (rows, row.shape[1]), 1)
    line = lax.broadcasted_iota(jnp.int32, (rows, row.shape[1]), 0)
    return jnp.sum(jnp.where(lanes == piece * rows + line, row, 0.0), axis=1, keepdims=True)


def dense_kernel(
    tokens_ref, gain_ref, ids_ref, route_ref, gate_hbm, up_hbm, down_hbm,
    out_ref,
    tok, part, cbuf, ybuf, zbuf, acc, routes, gate, up, down,
    wsem, arrived, routed, shared, crossed, climbed, sent, rsent,
):
    rows, width = tokens_ref.shape
    piece_rows = rows // PIECES
    me = lax.axis_index("ep")
    z, y, c = me // 4, (me // 2) % 2, me % 2
    flipped = (z >= PLANES // 2).astype(jnp.int32)
    level = jnp.where(z >= PLANES // 2, PLANES - 1 - z, z)
    is_end = level == 0
    upward = 1 - 2 * flipped
    ypeer, cpeer = z * 4 + (1 - y) * 2 + c, z * 4 + y * 2 + 1 - c
    above, below = me + 4 * upward, me - 4 * upward

    def plane_of(h):
        return jnp.where(z >= PLANES // 2, PLANES - 1 - h, h)

    def column_of(o):
        return jnp.where(o == 0, y, 1 - y)

    def remote(source, target, send_sem, recv_sem, device):
        return pltpu.make_async_remote_copy(
            src_ref=source, dst_ref=target, send_sem=send_sem, recv_sem=recv_sem,
            device_id={"ep": device}, device_id_type=MESH,
        )

    def move(kind, slot, device):
        return remote(tok.at[slot], tok.at[slot], sent.at[kind], arrived.at[slot], device)

    def move_route(kind, block, device):
        return remote(
            routes.at[block], routes.at[block], rsent.at[kind], routed.at[block], device
        )

    def hand(kind, slot, block, first, device):
        move(kind, slot, device).start()
        pl.when(first)(lambda: move_route(kind, block, device).start())

    weight_loads = [
        pltpu.make_async_copy(gate_hbm.at[0], gate, wsem.at[0]),
        pltpu.make_async_copy(up_hbm.at[0], up, wsem.at[1]),
        pltpu.make_async_copy(down_hbm.at[0], down, wsem.at[2]),
    ]
    for load in weight_loads:
        load.start()

    barrier = pltpu.get_barrier_semaphore()

    def greet(device):
        pl.semaphore_signal(barrier, inc=1, device_id={"ep": device}, device_id_type=MESH)

    greet(ypeer)
    greet(cpeer)
    greet(above)
    pl.when(jnp.logical_not(is_end))(lambda: greet(below))

    for e in range(PLANES):
        routes[me, e : e + 1, :] = jnp.sum(
            jnp.where(ids_ref[...] == e, route_ref[...], 0.0), axis=0, keepdims=True
        )

    def open_step(s, _):
        span = pl.ds(pl.multiple_of(s * piece_rows, piece_rows), piece_rows)
        values = tokens_ref[span, :].astype(jnp.float32)
        center = values - jnp.mean(values, axis=-1, keepdims=True)
        spread = jnp.mean(center * center, axis=-1, keepdims=True)
        slot = me * PIECES + s
        tok[slot] = (center * lax.rsqrt(spread + EPSILON) * gain_ref[...]).astype(jnp.bfloat16)

        @pl.when(s == 0)
        def _():
            pl.semaphore_wait(barrier, jnp.where(is_end, 3, 4))

        hand(1, slot, me, s == 0, above)
        pl.when(jnp.logical_not(is_end))(lambda: hand(2, slot, me, s == 0, below))
        hand(3, slot, me, s == 0, cpeer)
        return 0

    lax.fori_loop(0, PIECES, open_step, 0)
    for load in weight_loads:
        load.wait()

    def relay(h, o, s, entry):
        block = plane_of(h) * 4 + column_of(o) * 2 + c
        slot = block * PIECES + s
        move(3, slot, cpeer).wait_recv()
        pl.when(s == 0)(lambda: move_route(3, block, cpeer).wait_recv())
        pl.when((entry >> 8) & 1 == 1)(lambda: hand(1, slot, block, s == 0, above))
        pl.when((entry >> 9) & 1 == 1)(lambda: hand(2, slot, block, s == 0, below))
        hand(3, slot, block, s == 0, cpeer)

    def cross(h, s):
        block = plane_of(h) * 4 + y * 2 + c
        hand(0, block * PIECES + s, block, s == 0, ypeer)

    def share(pair, s):
        return remote(
            part.at[(pair * 2 + 1 - c) * PIECES + s], cbuf.at[pair * PIECES + s],
            sent.at[4], shared.at[pair * PIECES + s], cpeer,
        )

    def compute(h, o, s, entry):
        h2, o2, s2 = (entry >> 8) & 3, (entry >> 10) & 1, (entry >> 11) & 3
        pairs = [(plane_of(h) * 2 + column_of(o), s), (plane_of(h2) * 2 + column_of(o2), s2)]
        for n, (pair, piece) in enumerate(pairs):
            block = pair * 2 + 1 - c
            move(3, block * PIECES + piece, cpeer).wait_recv()
            pl.when((entry >> (13 + n)) & 1 == 1)(
                lambda block=block: move_route(3, block, cpeer).wait_recv()
            )
        places = [
            ((pair * 2 + core) * PIECES + piece, pair * 2 + core, piece)
            for pair, piece in pairs
            for core in range(2)
        ]
        x = jnp.concatenate([tok[slot] for slot, _, _ in places], axis=0)
        scale = jnp.concatenate(
            [
                lane_column(routes[block, pl.ds(z, 1), :], piece, piece_rows)
                for _, block, piece in places
            ],
            axis=0,
        )
        gate_cut = jnp.minimum(
            jnp.dot(x, gate[...], preferred_element_type=jnp.float32), clamp_limit
        )
        up_cut = jnp.clip(
            jnp.dot(x, up[...], preferred_element_type=jnp.float32), -clamp_limit, clamp_limit
        )
        active = ((up_cut + 1.0) * (gate_cut * jax.nn.sigmoid(gate_cut * sigmoid_slope))).astype(
            jnp.bfloat16
        )
        tile = min(512, width)
        for start in range(0, width, tile):
            value = scale * jnp.dot(
                active, down[:, start : start + tile], preferred_element_type=jnp.float32
            )
            value = value.astype(jnp.bfloat16)
            for n, (slot, _, _) in enumerate(places):
                part[slot, :, start : start + tile] = value[n * piece_rows : (n + 1) * piece_rows]
        for pair, piece in pairs:
            share(pair, piece).start()

    def settle(h, o, s, entry):
        plane = plane_of(h)
        pair = plane * 2 + column_of(o)
        slot = (pair * 2 + c) * PIECES + s
        rank = (plane * 2 + o) * PIECES + s
        lane = pair * PIECES + s
        row = plane * PIECES + s
        share(pair, s).wait_recv()
        acc[...] = part[slot].astype(jnp.float32) + cbuf[lane].astype(jnp.float32)

        def upon(side):
            return side * (2 * PLANES * PIECES) + rank

        def climb(side, device):
            return remote(
                part.at[slot], zbuf.at[upon(side)], sent.at[5], climbed.at[upon(side)], device
            )

        def over():
            return remote(part.at[slot], ybuf.at[row], sent.at[5], crossed.at[row], ypeer)

        @pl.when((entry >> 8) & 1 == 1)
        def _():
            over().wait_recv()
            acc[...] += ybuf[row].astype(jnp.float32)

        for bit, side, device in ((9, 1 - flipped, above), (10, flipped, below)):
            @pl.when((entry >> bit) & 1 == 1)
            def _():
                climb(side, device).wait_recv()
                acc[...] += zbuf[upon(side)].astype(jnp.float32)

        goal = (entry >> 11) & 3

        @pl.when(goal == 3)
        def _():
            out_ref[pl.ds(pl.multiple_of(s * piece_rows, piece_rows), piece_rows), :] = (
                acc[...].astype(jnp.bfloat16)
            )

        @pl.when(goal != 3)
        def _():
            part[slot] = acc[...].astype(jnp.bfloat16)

        pl.when(goal == 0)(lambda: over().start())
        pl.when(goal == 1)(lambda: climb(flipped, above).start())
        pl.when(goal == 2)(lambda: climb(1 - flipped, below).start())

    groups = max(len(END_WORDS), len(MID_WORDS)) // (GROUP // 2)

    def group_step(g, _):
        words = []
        for n in range(GROUP // 2):
            word = jnp.where(is_end, END_WORDS[n], MID_WORDS[n])
            for k in range(1, groups):
                at = k * (GROUP // 2) + n
                word = jnp.where(g == k, jnp.where(is_end, END_WORDS[at], MID_WORDS[at]), word)
            words.append(word)

        def entry_step(j, _):
            word = words[0]
            for n in range(1, GROUP // 2):
                word = jnp.where(j // 2 == n, words[n], word)
            entry = jnp.where(j % 2 == 0, word & 32767, word >> 15)
            kind = entry & 7
            h, o, s = (entry >> 3) & 3, (entry >> 5) & 1, (entry >> 6) & 3
            pl.when(kind == RELAY)(lambda: relay(h, o, s, entry))
            pl.when(kind == CROSS)(lambda: cross(h, s))
            pl.when(kind == COMPUTE)(lambda: compute(h, o, s, entry))
            pl.when(kind == SETTLE)(lambda: settle(h, o, s, entry))
            return 0

        lax.fori_loop(0, GROUP, entry_step, 0)
        return 0

    lax.fori_loop(0, groups, group_step, 0)

    def drain(counts, tiles):
        for kind, count in enumerate(counts):
            if count:
                whole = tok.at[pl.ds(0, count)]
                pltpu.make_async_copy(whole, whole, sent.at[kind]).wait()
        for kind, count in enumerate(tiles):
            if count:
                whole = routes.at[pl.ds(0, count)]
                pltpu.make_async_copy(whole, whole, rsent.at[kind]).wait()

    pl.when(is_end)(lambda: drain(END_SENT, END_TILES))
    pl.when(jnp.logical_not(is_end))(lambda: drain(MID_SENT, MID_TILES))


def dense_body(tokens, norm_gain, expert_ids, route_weight, gate_weight, up_weight, down_weight):
    devices = lax.axis_size("ep")
    rows, width = tokens.shape
    hidden = gate_weight.shape[2]
    piece_rows = rows // PIECES
    vmem, dma = pltpu.VMEM, pltpu.SemaphoreType.DMA
    block = jnp.bfloat16
    lanes = devices // 2 * PIECES
    return pl.pallas_call(
        dense_kernel,
        out_shape=jax.ShapeDtypeStruct((rows, width), block),
        in_specs=[pl.BlockSpec(memory_space=vmem)] * 4 + [pl.BlockSpec(memory_space=pl.ANY)] * 3,
        out_specs=pl.BlockSpec(memory_space=vmem),
        scratch_shapes=[
            vmem((devices * PIECES, piece_rows, width), block),
            vmem((devices * PIECES, piece_rows, width), block),
            vmem((lanes, piece_rows, width), block),
            vmem((PLANES * PIECES, piece_rows, width), block),
            vmem((4 * PLANES * PIECES, piece_rows, width), block),
            vmem((piece_rows, width), jnp.float32),
            vmem((devices, 8, rows), jnp.float32),
            vmem((width, hidden), block),
            vmem((width, hidden), block),
            vmem((hidden, width), block),
            dma((3,)),
            dma((devices * PIECES,)),
            dma((devices,)),
            dma((lanes,)),
            dma((PLANES * PIECES,)),
            dma((4 * PLANES * PIECES,)),
            dma((6,)),
            dma((4,)),
        ],
        compiler_params=pltpu.CompilerParams(
            collective_id=0, has_side_effects=True, vmem_limit_bytes=60 * 1024 * 1024
        ),
        name="dense_experts",
    )(
        tokens, norm_gain.reshape(1, width), expert_ids.T, route_weight.T,
        gate_weight, up_weight, down_weight,
    )


def body(tokens, norm_gain, expert_ids, route_weight, gate_weight, up_weight, down_weight):
    tok_rows, top_count = expert_ids.shape
    experts = lax.axis_size("ep") // SPLIT
    capacity = min(tok_rows, 2 * tok_rows * top_count // experts)
    dense = capacity == tok_rows and experts == PLANES and tok_rows % (16 * PIECES) == 0
    chosen = dense_body if dense else slot_body
    return chosen(
        tokens, norm_gain, expert_ids, route_weight, gate_weight, up_weight, down_weight
    )


def solution(mesh):
    placed = (
        P(("grp", "ep"), None),
        P(),
        P(("grp", "ep"), None),
        P(("grp", "ep"), None),
        P("ep", None, None),
        P("ep", None, None),
        P("ep", None, None),
    )
    return jax.shard_map(
        body, mesh=mesh, in_specs=placed, out_specs=P(("grp", "ep"), None), check_vma=False
    )
```

```python
import functools

import jax
import jax.numpy as jnp
from jax import lax
from jax.experimental import pallas as pl
from jax.experimental.pallas import tpu as pltpu
from jax.sharding import PartitionSpec as P

SPLIT = 4


EPSILON = 1e-05
clamp_limit = 7.0
sigmoid_slope = 1.702


def swapped(array, axis, bit):
    return lax.ppermute(array, axis, [(i, i ^ 1 << bit) for i in range(lax.axis_size(axis))])


def layer_norm(tokens, norm_gain):
    values = tokens.astype(jnp.float32)
    center = values - jnp.mean(values, axis=-1, keepdims=True)
    spread = jnp.mean(center * center, axis=-1, keepdims=True)
    return (center * lax.rsqrt(spread + EPSILON) * norm_gain).astype(jnp.bfloat16)


def expert_rows(block_rows, gate_weight, up_weight, down_weight):
    gate_pre = jnp.einsum(
        "scd,df->scf", block_rows, gate_weight[0], preferred_element_type=jnp.float32
    )
    up_pre = jnp.einsum("scd,df->scf", block_rows, up_weight[0], preferred_element_type=jnp.float32)
    gate_cut = jnp.minimum(gate_pre, clamp_limit)
    up_cut = jnp.clip(up_pre, -clamp_limit, clamp_limit)
    active = ((up_cut + 1.0) * (gate_cut * jax.nn.sigmoid(gate_cut * sigmoid_slope))).astype(
        jnp.bfloat16
    )
    return jnp.einsum("scf,fd->scd", active, down_weight[0], preferred_element_type=jnp.float32)


def slot_body(tokens, norm_gain, expert_ids, route_weight, gate_weight, up_weight, down_weight):
    normed = layer_norm(tokens, norm_gain)
    devices = lax.axis_size("ep")
    experts = devices // SPLIT
    tok_rows = tokens.shape[0]
    top_count = expert_ids.shape[1]
    width = tokens.shape[1]
    capacity = min(tok_rows, 2 * tok_rows * top_count // experts)
    quarter = capacity // SPLIT
    levels = SPLIT.bit_length() - 1
    position = lax.axis_index("ep")
    flat_ids = expert_ids.reshape(-1)
    onehot = (flat_ids[:, None] == jnp.arange(experts, dtype=jnp.int32)[None, :]).astype(jnp.int32)
    earlier = jnp.cumsum(onehot, axis=0) - onehot
    slot_index = jnp.sum(earlier * onehot, axis=1)
    target = flat_ids * capacity + slot_index
    owners = jnp.arange(flat_ids.shape[0], dtype=jnp.int32) // top_count
    slot_token = jnp.full((experts * capacity,), tok_rows, jnp.int32).at[target].set(owners)
    padded = jnp.concatenate([normed, jnp.zeros((1, width), jnp.bfloat16)], axis=0)
    outgoing = jnp.take(padded, slot_token, axis=0).reshape(experts, capacity, width)
    pieces = outgoing.reshape(devices, quarter, width)
    gathered = lax.all_to_all(pieces, "ep", split_axis=0, concat_axis=0, tiled=True)
    for bit_level in range(levels):
        partner = swapped(gathered, "ep", bit_level)
        upper_bit = position >> bit_level & 1
        first_half = jnp.where(upper_bit == 1, partner, gathered)
        second_half = jnp.where(upper_bit == 1, gathered, partner)
        gathered = jnp.concatenate([first_half, second_half], axis=1)
    partial_value = expert_rows(gathered, gate_weight, up_weight, down_weight)
    length = capacity
    for bit_level in reversed(range(levels)):
        length = length // 2
        upper_bit = position >> bit_level & 1
        kept_rows = lax.dynamic_slice_in_dim(partial_value, upper_bit * length, length, 1)
        sent_rows = lax.dynamic_slice_in_dim(partial_value, (1 - upper_bit) * length, length, 1)
        partial_value = kept_rows + swapped(sent_rows, "ep", bit_level)
    finished = partial_value.astype(jnp.bfloat16)
    returned = lax.all_to_all(finished, "ep", split_axis=0, concat_axis=0, tiled=True)
    results = returned.reshape(experts * capacity, width)
    picked = jnp.take(results, target, axis=0).reshape(tok_rows, top_count, width)
    combined = jnp.sum(route_weight[:, :, None] * picked.astype(jnp.float32), axis=1)
    return combined.astype(jnp.bfloat16)


MESH = pl.DeviceIdType.MESH
PLANES = 4
PIECES = 4

RELAY, CROSS, COMPUTE, SETTLE = 0, 1, 2, 3
GROUP = 8
END_WORDS = (
    32897, 262209, 335609865, 2373642, 13631520, 11534409,
    6341706, 1312779, 557072, 69566664, 6612242, 7340112,
    3408008, 67731480, 170459161, 68517936, 7110872, 2657386,
    69828745, 300744936, 1837163, 5347714, 8126648, 74311474,
    6815864, 201130096, 68780272, 121438267, 75333784, 259063995,
    4032627, 166264920, 5767411, 1149211, 98109851, 5505168,
    5870058, 82413915, 7706002, 80314539, 82150115, 80052835,
    230791939, 228694979,
)
MID_WORDS = (
    6586377, 8388648, 279248897, 557584, 19411242, 14680201,
    6340810, 17563680, 7602592, 11534361, 1573592, 23606306,
    10485969, 300744921, 2654264, 22806912, 20709800, 245965522,
    101297978, 24641609, 5344442, 69042424, 3670680, 7700704,
    103388610, 3408472, 326697648, 21495931, 6131811, 263785691,
    102335011, 108893786, 239927539, 104436419, 111216171, 5868571,
    158438018, 53841307, 112041739, 115970819, 5608323, 113876811,
    266703427, 139147,
)
END_SENT = (12, 6, 0, 32, 32, 28)
END_TILES = (4, 1, 0, 8)
MID_SENT = (11, 11, 16, 32, 32, 28)
MID_TILES = (4, 2, 3, 8)


def lane_column(row, piece, rows):
    lanes = lax.broadcasted_iota(jnp.int32, (rows, row.shape[1]), 1)
    line = lax.broadcasted_iota(jnp.int32, (rows, row.shape[1]), 0)
    return jnp.sum(jnp.where(lanes == piece * rows + line, row, 0.0), axis=1, keepdims=True)


def dense_kernel(
    tokens_hbm, gain_hbm, ids_hbm, route_hbm, gate_hbm, up_hbm, down_hbm,
    out_ref,
    tok, part, cbuf, ybuf, zbuf, acc, routes, tokens, gain, ids, route, gate, up, down,
    lsem, wsem, arrived, routed, shared, crossed, climbed, sent, rsent,
):
    rows, width = tokens_hbm.shape
    piece_rows = rows // PIECES
    me = lax.axis_index("ep")
    z, y, c = me // 4, (me // 2) % 2, me % 2
    flipped = (z >= PLANES // 2).astype(jnp.int32)
    level = jnp.where(z >= PLANES // 2, PLANES - 1 - z, z)
    is_end = level == 0
    upward = 1 - 2 * flipped
    ypeer, cpeer = z * 4 + (1 - y) * 2 + c, z * 4 + y * 2 + 1 - c
    above, below = me + 4 * upward, me - 4 * upward

    def plane_of(h):
        return jnp.where(z >= PLANES // 2, PLANES - 1 - h, h)

    def column_of(o):
        return jnp.where(o == 0, y, 1 - y)

    def remote(source, target, send_sem, recv_sem, device):
        return pltpu.make_async_remote_copy(
            src_ref=source, dst_ref=target, send_sem=send_sem, recv_sem=recv_sem,
            device_id={"ep": device}, device_id_type=MESH,
        )

    def move(kind, slot, device):
        return remote(tok.at[slot], tok.at[slot], sent.at[kind], arrived.at[slot], device)

    def move_route(kind, block, device):
        return remote(
            routes.at[block], routes.at[block], rsent.at[kind], routed.at[block], device
        )

    def hand(kind, slot, block, first, device):
        move(kind, slot, device).start()
        pl.when(first)(lambda: move_route(kind, block, device).start())

    barrier = pltpu.get_barrier_semaphore()

    def greet(device):
        pl.semaphore_signal(barrier, inc=1, device_id={"ep": device}, device_id_type=MESH)

    greet(ypeer)
    greet(cpeer)
    greet(above)
    pl.when(jnp.logical_not(is_end))(lambda: greet(below))

    def load_piece(s):
        span = pl.ds(pl.multiple_of(s * piece_rows, piece_rows), piece_rows)
        return pltpu.make_async_copy(tokens_hbm.at[span], tokens.at[span], wsem.at[s])

    small_loads = [
        pltpu.make_async_copy(ids_hbm, ids, lsem.at[0]),
        pltpu.make_async_copy(route_hbm, route, lsem.at[1]),
        pltpu.make_async_copy(gain_hbm, gain, lsem.at[2]),
    ]
    weight_loads = [
        pltpu.make_async_copy(gate_hbm.at[0], gate, lsem.at[3]),
        pltpu.make_async_copy(up_hbm.at[0], up, lsem.at[4]),
        pltpu.make_async_copy(down_hbm.at[0], down, lsem.at[5]),
    ]
    for s in range(PIECES):
        load_piece(s).start()
    for load in small_loads + weight_loads:
        load.start()

    for load in small_loads:
        load.wait()
    for e in range(PLANES):
        routes[me, e : e + 1, :] = jnp.sum(
            jnp.where(ids[...] == e, route[...], 0.0), axis=0, keepdims=True
        )

    def open_step(s, _):
        span = pl.ds(pl.multiple_of(s * piece_rows, piece_rows), piece_rows)
        load_piece(s).wait()
        values = tokens[span, :].astype(jnp.float32)
        center = values - jnp.mean(values, axis=-1, keepdims=True)
        spread = jnp.mean(center * center, axis=-1, keepdims=True)
        slot = me * PIECES + s
        tok[slot] = (center * lax.rsqrt(spread + EPSILON) * gain[...]).astype(jnp.bfloat16)

        @pl.when(s == 0)
        def _():
            pl.semaphore_wait(barrier, jnp.where(is_end, 3, 4))

        hand(1, slot, me, s == 0, above)
        pl.when(jnp.logical_not(is_end))(lambda: hand(2, slot, me, s == 0, below))
        hand(3, slot, me, s == 0, cpeer)
        return 0

    lax.fori_loop(0, PIECES, open_step, 0)
    for load in weight_loads:
        load.wait()

    def relay(h, o, s, entry):
        block = plane_of(h) * 4 + column_of(o) * 2 + c
        slot = block * PIECES + s
        move(3, slot, cpeer).wait_recv()
        pl.when(s == 0)(lambda: move_route(3, block, cpeer).wait_recv())
        pl.when((entry >> 8) & 1 == 1)(lambda: hand(1, slot, block, s == 0, above))
        pl.when((entry >> 9) & 1 == 1)(lambda: hand(2, slot, block, s == 0, below))
        hand(3, slot, block, s == 0, cpeer)

    def cross(h, s):
        block = plane_of(h) * 4 + y * 2 + c
        hand(0, block * PIECES + s, block, s == 0, ypeer)

    def share(pair, s):
        return remote(
            part.at[(pair * 2 + 1 - c) * PIECES + s], cbuf.at[pair * PIECES + s],
            sent.at[4], shared.at[pair * PIECES + s], cpeer,
        )

    def compute(h, o, s, entry):
        h2, o2, s2 = (entry >> 8) & 3, (entry >> 10) & 1, (entry >> 11) & 3
        pairs = [(plane_of(h) * 2 + column_of(o), s), (plane_of(h2) * 2 + column_of(o2), s2)]
        for n, (pair, piece) in enumerate(pairs):
            block = pair * 2 + 1 - c
            move(3, block * PIECES + piece, cpeer).wait_recv()
            pl.when((entry >> (13 + n)) & 1 == 1)(
                lambda block=block: move_route(3, block, cpeer).wait_recv()
            )
        places = [
            ((pair * 2 + core) * PIECES + piece, pair * 2 + core, piece)
            for pair, piece in pairs
            for core in range(2)
        ]
        x = jnp.concatenate([tok[slot] for slot, _, _ in places], axis=0)
        scale = jnp.concatenate(
            [
                lane_column(routes[block, pl.ds(z, 1), :], piece, piece_rows)
                for _, block, piece in places
            ],
            axis=0,
        )
        gate_cut = jnp.minimum(
            jnp.dot(x, gate[...], preferred_element_type=jnp.float32), clamp_limit
        )
        up_cut = jnp.clip(
            jnp.dot(x, up[...], preferred_element_type=jnp.float32), -clamp_limit, clamp_limit
        )
        active = ((up_cut + 1.0) * (gate_cut * jax.nn.sigmoid(gate_cut * sigmoid_slope))).astype(
            jnp.bfloat16
        )
        tile = min(512, width)
        for start in range(0, width, tile):
            value = scale * jnp.dot(
                active, down[:, start : start + tile], preferred_element_type=jnp.float32
            )
            value = value.astype(jnp.bfloat16)
            for n, (slot, _, _) in enumerate(places):
                part[slot, :, start : start + tile] = value[n * piece_rows : (n + 1) * piece_rows]
        for pair, piece in pairs:
            share(pair, piece).start()

    def settle(h, o, s, entry):
        plane = plane_of(h)
        pair = plane * 2 + column_of(o)
        slot = (pair * 2 + c) * PIECES + s
        rank = (plane * 2 + o) * PIECES + s
        lane = pair * PIECES + s
        row = plane * PIECES + s
        share(pair, s).wait_recv()
        acc[...] = part[slot].astype(jnp.float32) + cbuf[lane].astype(jnp.float32)

        def upon(side):
            return side * (2 * PLANES * PIECES) + rank

        def climb(side, device):
            return remote(
                part.at[slot], zbuf.at[upon(side)], sent.at[5], climbed.at[upon(side)], device
            )

        def over():
            return remote(part.at[slot], ybuf.at[row], sent.at[5], crossed.at[row], ypeer)

        @pl.when((entry >> 8) & 1 == 1)
        def _():
            over().wait_recv()
            acc[...] += ybuf[row].astype(jnp.float32)

        for bit, side, device in ((9, 1 - flipped, above), (10, flipped, below)):
            @pl.when((entry >> bit) & 1 == 1)
            def _():
                climb(side, device).wait_recv()
                acc[...] += zbuf[upon(side)].astype(jnp.float32)

        goal = (entry >> 11) & 3

        @pl.when(goal == 3)
        def _():
            out_ref[pl.ds(pl.multiple_of(s * piece_rows, piece_rows), piece_rows), :] = (
                acc[...].astype(jnp.bfloat16)
            )

        @pl.when(goal != 3)
        def _():
            part[slot] = acc[...].astype(jnp.bfloat16)

        pl.when(goal == 0)(lambda: over().start())
        pl.when(goal == 1)(lambda: climb(flipped, above).start())
        pl.when(goal == 2)(lambda: climb(1 - flipped, below).start())

    groups = max(len(END_WORDS), len(MID_WORDS)) // (GROUP // 2)

    def group_step(g, _):
        words = []
        for n in range(GROUP // 2):
            word = jnp.where(is_end, END_WORDS[n], MID_WORDS[n])
            for k in range(1, groups):
                at = k * (GROUP // 2) + n
                word = jnp.where(g == k, jnp.where(is_end, END_WORDS[at], MID_WORDS[at]), word)
            words.append(word)

        def entry_step(j, _):
            word = words[0]
            for n in range(1, GROUP // 2):
                word = jnp.where(j // 2 == n, words[n], word)
            entry = jnp.where(j % 2 == 0, word & 32767, word >> 15)
            kind = entry & 7
            h, o, s = (entry >> 3) & 3, (entry >> 5) & 1, (entry >> 6) & 3
            pl.when(kind == RELAY)(lambda: relay(h, o, s, entry))
            pl.when(kind == CROSS)(lambda: cross(h, s))
            pl.when(kind == COMPUTE)(lambda: compute(h, o, s, entry))
            pl.when(kind == SETTLE)(lambda: settle(h, o, s, entry))
            return 0

        lax.fori_loop(0, GROUP, entry_step, 0)
        return 0

    lax.fori_loop(0, groups, group_step, 0)

    def drain(counts, tiles):
        for kind, count in enumerate(counts):
            if count:
                whole = tok.at[pl.ds(0, count)]
                pltpu.make_async_copy(whole, whole, sent.at[kind]).wait()
        for kind, count in enumerate(tiles):
            if count:
                whole = routes.at[pl.ds(0, count)]
                pltpu.make_async_copy(whole, whole, rsent.at[kind]).wait()

    pl.when(is_end)(lambda: drain(END_SENT, END_TILES))
    pl.when(jnp.logical_not(is_end))(lambda: drain(MID_SENT, MID_TILES))


def dense_body(tokens, norm_gain, expert_ids, route_weight, gate_weight, up_weight, down_weight):
    devices = lax.axis_size("ep")
    rows, width = tokens.shape
    top = expert_ids.shape[1]
    hidden = gate_weight.shape[2]
    piece_rows = rows // PIECES
    vmem, dma = pltpu.VMEM, pltpu.SemaphoreType.DMA
    block = jnp.bfloat16
    lanes = devices // 2 * PIECES
    return pl.pallas_call(
        dense_kernel,
        out_shape=jax.ShapeDtypeStruct((rows, width), block),
        in_specs=[pl.BlockSpec(memory_space=pltpu.HBM)] * 7,
        out_specs=pl.BlockSpec(memory_space=vmem),
        scratch_shapes=[
            vmem((devices * PIECES, piece_rows, width), block),
            vmem((devices * PIECES, piece_rows, width), block),
            vmem((lanes, piece_rows, width), block),
            vmem((PLANES * PIECES, piece_rows, width), block),
            vmem((4 * PLANES * PIECES, piece_rows, width), block),
            vmem((piece_rows, width), jnp.float32),
            vmem((devices, 8, rows), jnp.float32),
            vmem((rows, width), block),
            vmem((1, width), jnp.float32),
            vmem((top, rows), jnp.int32),
            vmem((top, rows), jnp.float32),
            vmem((width, hidden), block),
            vmem((width, hidden), block),
            vmem((hidden, width), block),
            dma((6,)),
            dma((PIECES,)),
            dma((devices * PIECES,)),
            dma((devices,)),
            dma((lanes,)),
            dma((PLANES * PIECES,)),
            dma((4 * PLANES * PIECES,)),
            dma((6,)),
            dma((4,)),
        ],
        compiler_params=pltpu.CompilerParams(
            collective_id=0, has_side_effects=True, vmem_limit_bytes=40 * 1024 * 1024
        ),
        name="dense_experts",
    )(
        *[
            pltpu.with_memory_space_constraint(array, pltpu.HBM)
            for array in (
                tokens, norm_gain.reshape(1, width), expert_ids.T, route_weight.T,
                gate_weight, up_weight, down_weight,
            )
        ]
    )


def body(tokens, norm_gain, expert_ids, route_weight, gate_weight, up_weight, down_weight):
    tok_rows, top_count = expert_ids.shape
    experts = lax.axis_size("ep") // SPLIT
    capacity = min(tok_rows, 2 * tok_rows * top_count // experts)
    dense = capacity == tok_rows and experts == PLANES and tok_rows % (16 * PIECES) == 0
    chosen = dense_body if dense else slot_body
    return chosen(
        tokens, norm_gain, expert_ids, route_weight, gate_weight, up_weight, down_weight
    )


def solution(mesh):
    placed = (
        P(("grp", "ep"), None),
        P(),
        P(("grp", "ep"), None),
        P(("grp", "ep"), None),
        P("ep", None, None),
        P("ep", None, None),
        P("ep", None, None),
    )
    return jax.shard_map(
        body, mesh=mesh, in_specs=placed, out_specs=P(("grp", "ep"), None), check_vma=False
    )
```

```python
import functools

import jax
import jax.numpy as jnp
from jax import lax
from jax.experimental import pallas as pl
from jax.experimental.pallas import tpu as pltpu
from jax.sharding import PartitionSpec as P

SPLIT = 4


EPSILON = 1e-05
clamp_limit = 7.0
sigmoid_slope = 1.702


def swapped(array, axis, bit):
    return lax.ppermute(array, axis, [(i, i ^ 1 << bit) for i in range(lax.axis_size(axis))])


def layer_norm(tokens, norm_gain):
    values = tokens.astype(jnp.float32)
    center = values - jnp.mean(values, axis=-1, keepdims=True)
    spread = jnp.mean(center * center, axis=-1, keepdims=True)
    return (center * lax.rsqrt(spread + EPSILON) * norm_gain).astype(jnp.bfloat16)


def expert_rows(block_rows, gate_weight, up_weight, down_weight):
    gate_pre = jnp.einsum(
        "scd,df->scf", block_rows, gate_weight[0], preferred_element_type=jnp.float32
    )
    up_pre = jnp.einsum("scd,df->scf", block_rows, up_weight[0], preferred_element_type=jnp.float32)
    gate_cut = jnp.minimum(gate_pre, clamp_limit)
    up_cut = jnp.clip(up_pre, -clamp_limit, clamp_limit)
    active = ((up_cut + 1.0) * (gate_cut * jax.nn.sigmoid(gate_cut * sigmoid_slope))).astype(
        jnp.bfloat16
    )
    return jnp.einsum("scf,fd->scd", active, down_weight[0], preferred_element_type=jnp.float32)


def slot_body(tokens, norm_gain, expert_ids, route_weight, gate_weight, up_weight, down_weight):
    normed = layer_norm(tokens, norm_gain)
    devices = lax.axis_size("ep")
    experts = devices // SPLIT
    tok_rows = tokens.shape[0]
    top_count = expert_ids.shape[1]
    width = tokens.shape[1]
    capacity = min(tok_rows, 2 * tok_rows * top_count // experts)
    quarter = capacity // SPLIT
    levels = SPLIT.bit_length() - 1
    position = lax.axis_index("ep")
    flat_ids = expert_ids.reshape(-1)
    onehot = (flat_ids[:, None] == jnp.arange(experts, dtype=jnp.int32)[None, :]).astype(jnp.int32)
    earlier = jnp.cumsum(onehot, axis=0) - onehot
    slot_index = jnp.sum(earlier * onehot, axis=1)
    target = flat_ids * capacity + slot_index
    owners = jnp.arange(flat_ids.shape[0], dtype=jnp.int32) // top_count
    slot_token = jnp.full((experts * capacity,), tok_rows, jnp.int32).at[target].set(owners)
    padded = jnp.concatenate([normed, jnp.zeros((1, width), jnp.bfloat16)], axis=0)
    outgoing = jnp.take(padded, slot_token, axis=0).reshape(experts, capacity, width)
    pieces = outgoing.reshape(devices, quarter, width)
    gathered = lax.all_to_all(pieces, "ep", split_axis=0, concat_axis=0, tiled=True)
    for bit_level in range(levels):
        partner = swapped(gathered, "ep", bit_level)
        upper_bit = position >> bit_level & 1
        first_half = jnp.where(upper_bit == 1, partner, gathered)
        second_half = jnp.where(upper_bit == 1, gathered, partner)
        gathered = jnp.concatenate([first_half, second_half], axis=1)
    partial_value = expert_rows(gathered, gate_weight, up_weight, down_weight)
    length = capacity
    for bit_level in reversed(range(levels)):
        length = length // 2
        upper_bit = position >> bit_level & 1
        kept_rows = lax.dynamic_slice_in_dim(partial_value, upper_bit * length, length, 1)
        sent_rows = lax.dynamic_slice_in_dim(partial_value, (1 - upper_bit) * length, length, 1)
        partial_value = kept_rows + swapped(sent_rows, "ep", bit_level)
    finished = partial_value.astype(jnp.bfloat16)
    returned = lax.all_to_all(finished, "ep", split_axis=0, concat_axis=0, tiled=True)
    results = returned.reshape(experts * capacity, width)
    picked = jnp.take(results, target, axis=0).reshape(tok_rows, top_count, width)
    combined = jnp.sum(route_weight[:, :, None] * picked.astype(jnp.float32), axis=1)
    return combined.astype(jnp.bfloat16)


MESH = pl.DeviceIdType.MESH
PLANES = 4
PIECES = 4

RELAY, CROSS, COMPUTE, SETTLE = 0, 1, 2, 3
GROUP = 8
END_WORDS = (
    2130049, 294920, 470099970, 1048648, 2392480, 572850528,
    67469505, 524328, 6553617, 847841355, 2621641, 4456672,
    786536, 821267, 1578066, 7079979, 104136921, 4489297,
    7604307, 70624218, 213975096, 6029475, 865665272, 3934427,
    3670224, 7870458, 1935411, 4984442, 6129915, 70885090,
    2883707, 7967698, 76382384, 80576547, 4721586, 150274216,
    78479539, 180947411, 5603563, 24218003, 20023755, 226593163,
    232889219, 138051,
)
MID_WORDS = (
    1310921, 33024, 17310026, 412418065, 4489808, 543490496,
    1048769, 13632024, 819432, 23855456, 437321776, 6849232,
    7110976, 1844186, 12582993, 13894328, 292094584, 396172626,
    2395155, 106758896, 8126627, 21760059, 7340144, 182517995,
    19663955, 22544488, 4040434, 137462416, 107839675, 17932146,
    187501619, 7965947, 157392026, 51743859, 101551426, 155254963,
    114135779, 260408939, 159485275, 163679699, 262504619, 153193875,
    264609739, 131076,
)
END_SENT = (12, 6, 0, 32, 32, 28)
END_TILES = (4, 1, 0, 8)
MID_SENT = (11, 11, 16, 32, 32, 28)
MID_TILES = (4, 2, 3, 8)


def lane_column(row, piece, rows):
    lanes = lax.broadcasted_iota(jnp.int32, (rows, row.shape[1]), 1)
    line = lax.broadcasted_iota(jnp.int32, (rows, row.shape[1]), 0)
    return jnp.sum(jnp.where(lanes == piece * rows + line, row, 0.0), axis=1, keepdims=True)


def dense_kernel(
    tokens_hbm, gain_hbm, ids_hbm, route_hbm, gate_hbm, up_hbm, down_hbm,
    out_ref,
    tok, part, cbuf, ybuf, zbuf, acc, routes, tokens, gain, ids, route, gate, up, down,
    lsem, wsem, arrived, routed, shared, crossed, climbed, sent, rsent,
):
    rows, width = tokens_hbm.shape
    piece_rows = rows // PIECES
    me = lax.axis_index("ep")
    z, y, c = me // 4, (me // 2) % 2, me % 2
    flipped = (z >= PLANES // 2).astype(jnp.int32)
    level = jnp.where(z >= PLANES // 2, PLANES - 1 - z, z)
    is_end = level == 0
    upward = 1 - 2 * flipped
    ypeer, cpeer = z * 4 + (1 - y) * 2 + c, z * 4 + y * 2 + 1 - c
    above, below = me + 4 * upward, me - 4 * upward

    def plane_of(h):
        return jnp.where(z >= PLANES // 2, PLANES - 1 - h, h)

    def column_of(o):
        return jnp.where(o == 0, y, 1 - y)

    def remote(source, target, send_sem, recv_sem, device):
        return pltpu.make_async_remote_copy(
            src_ref=source, dst_ref=target, send_sem=send_sem, recv_sem=recv_sem,
            device_id={"ep": device}, device_id_type=MESH,
        )

    def move(kind, slot, device):
        return remote(tok.at[slot], tok.at[slot], sent.at[kind], arrived.at[slot], device)

    def move_route(kind, block, device):
        return remote(
            routes.at[block], routes.at[block], rsent.at[kind], routed.at[block], device
        )

    def hand(kind, slot, block, first, device):
        move(kind, slot, device).start()
        pl.when(first)(lambda: move_route(kind, block, device).start())

    barrier = pltpu.get_barrier_semaphore()

    def greet(device):
        pl.semaphore_signal(barrier, inc=1, device_id={"ep": device}, device_id_type=MESH)

    greet(ypeer)
    greet(cpeer)
    greet(above)
    pl.when(jnp.logical_not(is_end))(lambda: greet(below))

    def load_piece(s):
        span = pl.ds(pl.multiple_of(s * piece_rows, piece_rows), piece_rows)
        return pltpu.make_async_copy(tokens_hbm.at[span], tokens.at[span], wsem.at[s])

    small_loads = [
        pltpu.make_async_copy(ids_hbm, ids, lsem.at[0]),
        pltpu.make_async_copy(route_hbm, route, lsem.at[1]),
        pltpu.make_async_copy(gain_hbm, gain, lsem.at[2]),
    ]
    weight_loads = [
        pltpu.make_async_copy(gate_hbm.at[0], gate, lsem.at[3]),
        pltpu.make_async_copy(up_hbm.at[0], up, lsem.at[4]),
        pltpu.make_async_copy(down_hbm.at[0], down, lsem.at[5]),
    ]
    for s in range(PIECES):
        load_piece(s).start()
    for load in small_loads + weight_loads:
        load.start()

    for load in small_loads:
        load.wait()
    for e in range(PLANES):
        routes[me, e : e + 1, :] = jnp.sum(
            jnp.where(ids[...] == e, route[...], 0.0), axis=0, keepdims=True
        )

    def open_step(s, _):
        span = pl.ds(pl.multiple_of(s * piece_rows, piece_rows), piece_rows)
        load_piece(s).wait()
        values = tokens[span, :].astype(jnp.float32)
        center = values - jnp.mean(values, axis=-1, keepdims=True)
        spread = jnp.mean(center * center, axis=-1, keepdims=True)
        slot = me * PIECES + s
        tok[slot] = (center * lax.rsqrt(spread + EPSILON) * gain[...]).astype(jnp.bfloat16)

        @pl.when(s == 0)
        def _():
            pl.semaphore_wait(barrier, jnp.where(is_end, 3, 4))

        hand(1, slot, me, s == 0, above)
        pl.when(jnp.logical_not(is_end))(lambda: hand(2, slot, me, s == 0, below))
        pl.when(s == 0)(lambda: hand(0, slot, me, True, ypeer))
        hand(3, slot, me, s == 0, cpeer)
        return 0

    lax.fori_loop(0, PIECES, open_step, 0)
    for load in weight_loads:
        load.wait()

    def relay(h, o, s, entry):
        block = plane_of(h) * 4 + column_of(o) * 2 + c
        slot = block * PIECES + s
        move(3, slot, cpeer).wait_recv()
        pl.when(s == 0)(lambda: move_route(3, block, cpeer).wait_recv())
        pl.when((entry >> 8) & 1 == 1)(lambda: hand(1, slot, block, s == 0, above))
        pl.when((entry >> 9) & 1 == 1)(lambda: hand(2, slot, block, s == 0, below))
        hand(3, slot, block, s == 0, cpeer)

    def cross(h, s):
        block = plane_of(h) * 4 + y * 2 + c
        hand(0, block * PIECES + s, block, s == 0, ypeer)

    def share(pair, s):
        return remote(
            part.at[(pair * 2 + 1 - c) * PIECES + s], cbuf.at[pair * PIECES + s],
            sent.at[4], shared.at[pair * PIECES + s], cpeer,
        )

    def compute(h, o, s, entry):
        h2, o2, s2 = (entry >> 8) & 3, (entry >> 10) & 1, (entry >> 11) & 3
        pairs = [(plane_of(h) * 2 + column_of(o), s), (plane_of(h2) * 2 + column_of(o2), s2)]
        for n, (pair, piece) in enumerate(pairs):
            block = pair * 2 + 1 - c
            move(3, block * PIECES + piece, cpeer).wait_recv()
            pl.when((entry >> (13 + n)) & 1 == 1)(
                lambda block=block: move_route(3, block, cpeer).wait_recv()
            )
        places = [
            ((pair * 2 + core) * PIECES + piece, pair * 2 + core, piece)
            for pair, piece in pairs
            for core in range(2)
        ]
        x = jnp.concatenate([tok[slot] for slot, _, _ in places], axis=0)
        scale = jnp.concatenate(
            [
                lane_column(routes[block, pl.ds(z, 1), :], piece, piece_rows)
                for _, block, piece in places
            ],
            axis=0,
        )
        gate_cut = jnp.minimum(
            jnp.dot(x, gate[...], preferred_element_type=jnp.float32), clamp_limit
        )
        up_cut = jnp.clip(
            jnp.dot(x, up[...], preferred_element_type=jnp.float32), -clamp_limit, clamp_limit
        )
        active = ((up_cut + 1.0) * (gate_cut * jax.nn.sigmoid(gate_cut * sigmoid_slope))).astype(
            jnp.bfloat16
        )
        tile = min(512, width)
        for start in range(0, width, tile):
            value = scale * jnp.dot(
                active, down[:, start : start + tile], preferred_element_type=jnp.float32
            )
            value = value.astype(jnp.bfloat16)
            for n, (slot, _, _) in enumerate(places):
                part[slot, :, start : start + tile] = value[n * piece_rows : (n + 1) * piece_rows]
        for pair, piece in pairs:
            share(pair, piece).start()

    def settle(h, o, s, entry):
        plane = plane_of(h)
        pair = plane * 2 + column_of(o)
        slot = (pair * 2 + c) * PIECES + s
        rank = (plane * 2 + o) * PIECES + s
        lane = pair * PIECES + s
        row = plane * PIECES + s
        share(pair, s).wait_recv()
        acc[...] = part[slot].astype(jnp.float32) + cbuf[lane].astype(jnp.float32)

        def upon(side):
            return side * (2 * PLANES * PIECES) + rank

        def climb(side, device):
            return remote(
                part.at[slot], zbuf.at[upon(side)], sent.at[5], climbed.at[upon(side)], device
            )

        def over():
            return remote(part.at[slot], ybuf.at[row], sent.at[5], crossed.at[row], ypeer)

        @pl.when((entry >> 8) & 1 == 1)
        def _():
            over().wait_recv()
            acc[...] += ybuf[row].astype(jnp.float32)

        for bit, side, device in ((9, 1 - flipped, above), (10, flipped, below)):
            @pl.when((entry >> bit) & 1 == 1)
            def _():
                climb(side, device).wait_recv()
                acc[...] += zbuf[upon(side)].astype(jnp.float32)

        goal = (entry >> 11) & 3

        @pl.when(goal == 3)
        def _():
            out_ref[pl.ds(pl.multiple_of(s * piece_rows, piece_rows), piece_rows), :] = (
                acc[...].astype(jnp.bfloat16)
            )

        @pl.when(goal != 3)
        def _():
            part[slot] = acc[...].astype(jnp.bfloat16)

        pl.when(goal == 0)(lambda: over().start())
        pl.when(goal == 1)(lambda: climb(flipped, above).start())
        pl.when(goal == 2)(lambda: climb(1 - flipped, below).start())

    groups = max(len(END_WORDS), len(MID_WORDS)) // (GROUP // 2)

    def group_step(g, _):
        words = []
        for n in range(GROUP // 2):
            word = jnp.where(is_end, END_WORDS[n], MID_WORDS[n])
            for k in range(1, groups):
                at = k * (GROUP // 2) + n
                word = jnp.where(g == k, jnp.where(is_end, END_WORDS[at], MID_WORDS[at]), word)
            words.append(word)

        def entry_step(j, _):
            word = words[0]
            for n in range(1, GROUP // 2):
                word = jnp.where(j // 2 == n, words[n], word)
            entry = jnp.where(j % 2 == 0, word & 32767, word >> 15)
            kind = entry & 7
            h, o, s = (entry >> 3) & 3, (entry >> 5) & 1, (entry >> 6) & 3
            pl.when(kind == RELAY)(lambda: relay(h, o, s, entry))
            pl.when(kind == CROSS)(lambda: cross(h, s))
            pl.when(kind == COMPUTE)(lambda: compute(h, o, s, entry))
            pl.when(kind == SETTLE)(lambda: settle(h, o, s, entry))
            return 0

        lax.fori_loop(0, GROUP, entry_step, 0)
        return 0

    lax.fori_loop(0, groups, group_step, 0)

    def drain(counts, tiles):
        for kind, count in enumerate(counts):
            if count:
                whole = tok.at[pl.ds(0, count)]
                pltpu.make_async_copy(whole, whole, sent.at[kind]).wait()
        for kind, count in enumerate(tiles):
            if count:
                whole = routes.at[pl.ds(0, count)]
                pltpu.make_async_copy(whole, whole, rsent.at[kind]).wait()

    pl.when(is_end)(lambda: drain(END_SENT, END_TILES))
    pl.when(jnp.logical_not(is_end))(lambda: drain(MID_SENT, MID_TILES))


def dense_body(tokens, norm_gain, expert_ids, route_weight, gate_weight, up_weight, down_weight):
    devices = lax.axis_size("ep")
    rows, width = tokens.shape
    top = expert_ids.shape[1]
    hidden = gate_weight.shape[2]
    piece_rows = rows // PIECES
    vmem, dma = pltpu.VMEM, pltpu.SemaphoreType.DMA
    block = jnp.bfloat16
    lanes = devices // 2 * PIECES
    return pl.pallas_call(
        dense_kernel,
        out_shape=jax.ShapeDtypeStruct((rows, width), block),
        in_specs=[pl.BlockSpec(memory_space=pltpu.HBM)] * 7,
        out_specs=pl.BlockSpec(memory_space=vmem),
        scratch_shapes=[
            vmem((devices * PIECES, piece_rows, width), block),
            vmem((devices * PIECES, piece_rows, width), block),
            vmem((lanes, piece_rows, width), block),
            vmem((PLANES * PIECES, piece_rows, width), block),
            vmem((4 * PLANES * PIECES, piece_rows, width), block),
            vmem((piece_rows, width), jnp.float32),
            vmem((devices, PLANES, rows), jnp.float32),
            vmem((rows, width), block),
            vmem((1, width), jnp.float32),
            vmem((top, rows), jnp.int32),
            vmem((top, rows), jnp.float32),
            vmem((width, hidden), block),
            vmem((width, hidden), block),
            vmem((hidden, width), block),
            dma((6,)),
            dma((PIECES,)),
            dma((devices * PIECES,)),
            dma((devices,)),
            dma((lanes,)),
            dma((PLANES * PIECES,)),
            dma((4 * PLANES * PIECES,)),
            dma((6,)),
            dma((4,)),
        ],
        compiler_params=pltpu.CompilerParams(
            collective_id=0, has_side_effects=True, vmem_limit_bytes=40 * 1024 * 1024
        ),
        name="dense_experts",
    )(
        *[
            pltpu.with_memory_space_constraint(array, pltpu.HBM)
            for array in (
                tokens, norm_gain.reshape(1, width), expert_ids.T, route_weight.T,
                gate_weight, up_weight, down_weight,
            )
        ]
    )


def body(tokens, norm_gain, expert_ids, route_weight, gate_weight, up_weight, down_weight):
    tok_rows, top_count = expert_ids.shape
    experts = lax.axis_size("ep") // SPLIT
    capacity = min(tok_rows, 2 * tok_rows * top_count // experts)
    dense = capacity == tok_rows and experts == PLANES and tok_rows % (16 * PIECES) == 0
    chosen = dense_body if dense else slot_body
    return chosen(
        tokens, norm_gain, expert_ids, route_weight, gate_weight, up_weight, down_weight
    )


def solution(mesh):
    placed = (
        P(("grp", "ep"), None),
        P(),
        P(("grp", "ep"), None),
        P(("grp", "ep"), None),
        P("ep", None, None),
        P("ep", None, None),
        P("ep", None, None),
    )
    return jax.shard_map(
        body, mesh=mesh, in_specs=placed, out_specs=P(("grp", "ep"), None), check_vma=False
    )
```

```python
import functools

import jax
import jax.numpy as jnp
from jax import lax
from jax.experimental import pallas as pl
from jax.experimental.pallas import tpu as pltpu
from jax.sharding import PartitionSpec as P

SPLIT = 4


EPSILON = 1e-05
clamp_limit = 7.0
sigmoid_slope = 1.702


def swapped(array, axis, bit):
    return lax.ppermute(array, axis, [(i, i ^ 1 << bit) for i in range(lax.axis_size(axis))])


def layer_norm(tokens, norm_gain):
    values = tokens.astype(jnp.float32)
    center = values - jnp.mean(values, axis=-1, keepdims=True)
    spread = jnp.mean(center * center, axis=-1, keepdims=True)
    return (center * lax.rsqrt(spread + EPSILON) * norm_gain).astype(jnp.bfloat16)


def expert_rows(block_rows, gate_weight, up_weight, down_weight):
    gate_pre = jnp.einsum(
        "scd,df->scf", block_rows, gate_weight[0], preferred_element_type=jnp.float32
    )
    up_pre = jnp.einsum("scd,df->scf", block_rows, up_weight[0], preferred_element_type=jnp.float32)
    gate_cut = jnp.minimum(gate_pre, clamp_limit)
    up_cut = jnp.clip(up_pre, -clamp_limit, clamp_limit)
    active = ((up_cut + 1.0) * (gate_cut * jax.nn.sigmoid(gate_cut * sigmoid_slope))).astype(
        jnp.bfloat16
    )
    return jnp.einsum("scf,fd->scd", active, down_weight[0], preferred_element_type=jnp.float32)


def slot_body(tokens, norm_gain, expert_ids, route_weight, gate_weight, up_weight, down_weight):
    normed = layer_norm(tokens, norm_gain)
    devices = lax.axis_size("ep")
    experts = devices // SPLIT
    tok_rows = tokens.shape[0]
    top_count = expert_ids.shape[1]
    width = tokens.shape[1]
    capacity = min(tok_rows, 2 * tok_rows * top_count // experts)
    quarter = capacity // SPLIT
    levels = SPLIT.bit_length() - 1
    position = lax.axis_index("ep")
    flat_ids = expert_ids.reshape(-1)
    onehot = (flat_ids[:, None] == jnp.arange(experts, dtype=jnp.int32)[None, :]).astype(jnp.int32)
    earlier = jnp.cumsum(onehot, axis=0) - onehot
    slot_index = jnp.sum(earlier * onehot, axis=1)
    target = flat_ids * capacity + slot_index
    owners = jnp.arange(flat_ids.shape[0], dtype=jnp.int32) // top_count
    slot_token = jnp.full((experts * capacity,), tok_rows, jnp.int32).at[target].set(owners)
    padded = jnp.concatenate([normed, jnp.zeros((1, width), jnp.bfloat16)], axis=0)
    outgoing = jnp.take(padded, slot_token, axis=0).reshape(experts, capacity, width)
    pieces = outgoing.reshape(devices, quarter, width)
    gathered = lax.all_to_all(pieces, "ep", split_axis=0, concat_axis=0, tiled=True)
    for bit_level in range(levels):
        partner = swapped(gathered, "ep", bit_level)
        upper_bit = position >> bit_level & 1
        first_half = jnp.where(upper_bit == 1, partner, gathered)
        second_half = jnp.where(upper_bit == 1, gathered, partner)
        gathered = jnp.concatenate([first_half, second_half], axis=1)
    partial_value = expert_rows(gathered, gate_weight, up_weight, down_weight)
    length = capacity
    for bit_level in reversed(range(levels)):
        length = length // 2
        upper_bit = position >> bit_level & 1
        kept_rows = lax.dynamic_slice_in_dim(partial_value, upper_bit * length, length, 1)
        sent_rows = lax.dynamic_slice_in_dim(partial_value, (1 - upper_bit) * length, length, 1)
        partial_value = kept_rows + swapped(sent_rows, "ep", bit_level)
    finished = partial_value.astype(jnp.bfloat16)
    returned = lax.all_to_all(finished, "ep", split_axis=0, concat_axis=0, tiled=True)
    results = returned.reshape(experts * capacity, width)
    picked = jnp.take(results, target, axis=0).reshape(tok_rows, top_count, width)
    combined = jnp.sum(route_weight[:, :, None] * picked.astype(jnp.float32), axis=1)
    return combined.astype(jnp.bfloat16)


MESH = pl.DeviceIdType.MESH
PLANES = 4
PIECES = 4

RELAY, CROSS, COMPUTE, SETTLE = 0, 1, 2, 3
GROUP = 8
END_WORDS = (
    6324353, 1048584, 13631497, 4489352, 805634528, 148963393,
    67469352, 557072, 71689506, 2654288, 555810984, 819224,
    1574955, 67734242, 2916440, 592773320, 69828809, 3670072,
    7438544, 600901803, 6029432, 68797298, 8126523, 1153402,
    7866483, 608016378, 100204760, 3145979, 7604507, 5767355,
    346921690, 7962776, 82679530, 4721818, 5865544, 80576747,
    139001960, 111479251, 3508627, 82156291, 22127203, 232884555,
    230792003, 131076,
)
MID_WORDS = (
    8388809, 17301505, 805634065, 4489808, 2130240, 88418322,
    1048616, 819736, 1573280, 23593560, 2654688, 13893841,
    504181794, 7602272, 14680120, 22806912, 488177737, 2916464,
    1147640, 24641763, 23866426, 587009043, 207422128, 103383160,
    1933976, 96010896, 188811451, 8227891, 20191610, 256725091,
    306023539, 51748314, 109936883, 156340842, 81071451, 159482035,
    260410843, 39170883, 7703707, 115966571, 113873859, 266703491,
    262512523, 131076,
)
END_SENT = (11, 6, 0, 32, 32, 28)
END_TILES = (4, 1, 0, 8)
MID_SENT = (11, 11, 17, 32, 32, 28)
MID_TILES = (4, 2, 3, 8)


def lane_column(row, piece, rows):
    lanes = lax.broadcasted_iota(jnp.int32, (rows, row.shape[1]), 1)
    line = lax.broadcasted_iota(jnp.int32, (rows, row.shape[1]), 0)
    return jnp.sum(jnp.where(lanes == piece * rows + line, row, 0.0), axis=1, keepdims=True)


def dense_kernel(
    tokens_hbm, gain_hbm, ids_hbm, route_hbm, gate_hbm, up_hbm, down_hbm,
    out_ref,
    tok, part, cbuf, ybuf, zbuf, acc, routes, tokens, gain, ids, route, gate, up, down,
    lsem, wsem, arrived, routed, shared, crossed, climbed, sent, rsent,
):
    rows, width = tokens_hbm.shape
    piece_rows = rows // PIECES
    me = lax.axis_index("ep")
    z, y, c = me // 4, (me // 2) % 2, me % 2
    flipped = (z >= PLANES // 2).astype(jnp.int32)
    level = jnp.where(z >= PLANES // 2, PLANES - 1 - z, z)
    is_end = level == 0
    upward = 1 - 2 * flipped
    ypeer, cpeer = z * 4 + (1 - y) * 2 + c, z * 4 + y * 2 + 1 - c
    above, below = me + 4 * upward, me - 4 * upward

    def plane_of(h):
        return jnp.where(z >= PLANES // 2, PLANES - 1 - h, h)

    def column_of(o):
        return jnp.where(o == 0, y, 1 - y)

    def remote(source, target, send_sem, recv_sem, device):
        return pltpu.make_async_remote_copy(
            src_ref=source, dst_ref=target, send_sem=send_sem, recv_sem=recv_sem,
            device_id={"ep": device}, device_id_type=MESH,
        )

    def move(kind, slot, device):
        return remote(tok.at[slot], tok.at[slot], sent.at[kind], arrived.at[slot], device)

    def move_route(kind, block, device):
        return remote(
            routes.at[block], routes.at[block], rsent.at[kind], routed.at[block], device
        )

    def hand(kind, slot, block, first, device):
        move(kind, slot, device).start()
        pl.when(first)(lambda: move_route(kind, block, device).start())

    barrier = pltpu.get_barrier_semaphore()

    def greet(device):
        pl.semaphore_signal(barrier, inc=1, device_id={"ep": device}, device_id_type=MESH)

    greet(ypeer)
    greet(cpeer)
    greet(above)
    pl.when(jnp.logical_not(is_end))(lambda: greet(below))

    def load_piece(s):
        span = pl.ds(pl.multiple_of(s * piece_rows, piece_rows), piece_rows)
        return pltpu.make_async_copy(tokens_hbm.at[span], tokens.at[span], wsem.at[s])

    small_loads = [
        pltpu.make_async_copy(ids_hbm, ids, lsem.at[0]),
        pltpu.make_async_copy(route_hbm, route, lsem.at[1]),
        pltpu.make_async_copy(gain_hbm, gain, lsem.at[2]),
    ]
    weight_loads = [
        pltpu.make_async_copy(gate_hbm.at[0], gate, lsem.at[3]),
        pltpu.make_async_copy(up_hbm.at[0], up, lsem.at[4]),
        pltpu.make_async_copy(down_hbm.at[0], down, lsem.at[5]),
    ]
    for s in range(PIECES):
        load_piece(s).start()
    for load in small_loads + weight_loads:
        load.start()

    for load in small_loads:
        load.wait()
    for e in range(PLANES):
        routes[me, e : e + 1, :] = jnp.sum(
            jnp.where(ids[...] == e, route[...], 0.0), axis=0, keepdims=True
        )

    def open_step(s, _):
        span = pl.ds(pl.multiple_of(s * piece_rows, piece_rows), piece_rows)
        load_piece(s).wait()
        values = tokens[span, :].astype(jnp.float32)
        center = values - jnp.mean(values, axis=-1, keepdims=True)
        spread = jnp.mean(center * center, axis=-1, keepdims=True)
        slot = me * PIECES + s
        tok[slot] = (center * lax.rsqrt(spread + EPSILON) * gain[...]).astype(jnp.bfloat16)

        @pl.when(s == 0)
        def _():
            pl.semaphore_wait(barrier, jnp.where(is_end, 3, 4))

        hand(1, slot, me, s == 0, above)
        pl.when(jnp.logical_not(is_end))(lambda: hand(2, slot, me, s == 0, below))
        pl.when(s == 0)(lambda: hand(0, slot, me, True, ypeer))
        hand(3, slot, me, s == 0, cpeer)
        return 0

    lax.fori_loop(0, PIECES, open_step, 0)
    for load in weight_loads:
        load.wait()

    def relay(h, o, s, entry):
        block = plane_of(h) * 4 + column_of(o) * 2 + c
        slot = block * PIECES + s
        move(3, slot, cpeer).wait_recv()
        pl.when(s == 0)(lambda: move_route(3, block, cpeer).wait_recv())
        pl.when((entry >> 8) & 1 == 1)(lambda: hand(1, slot, block, s == 0, above))
        pl.when((entry >> 9) & 1 == 1)(lambda: hand(2, slot, block, s == 0, below))
        hand(3, slot, block, s == 0, cpeer)

    def cross(h, s):
        block = plane_of(h) * 4 + y * 2 + c
        hand(0, block * PIECES + s, block, s == 0, ypeer)

    def share(pair, s):
        return remote(
            part.at[(pair * 2 + 1 - c) * PIECES + s], cbuf.at[pair * PIECES + s],
            sent.at[4], shared.at[pair * PIECES + s], cpeer,
        )

    def compute(h, o, s, entry):
        h2, o2, s2 = (entry >> 8) & 3, (entry >> 10) & 1, (entry >> 11) & 3
        pairs = [(plane_of(h) * 2 + column_of(o), s), (plane_of(h2) * 2 + column_of(o2), s2)]
        for n, (pair, piece) in enumerate(pairs):
            block = pair * 2 + 1 - c
            move(3, block * PIECES + piece, cpeer).wait_recv()
            pl.when((entry >> (13 + n)) & 1 == 1)(
                lambda block=block: move_route(3, block, cpeer).wait_recv()
            )
        places = [
            ((pair * 2 + core) * PIECES + piece, pair * 2 + core, piece)
            for pair, piece in pairs
            for core in range(2)
        ]
        x = jnp.concatenate([tok[slot] for slot, _, _ in places], axis=0)
        scale = jnp.concatenate(
            [
                lane_column(routes[block, pl.ds(z, 1), :], piece, piece_rows)
                for _, block, piece in places
            ],
            axis=0,
        )
        gate_cut = jnp.minimum(
            jnp.dot(x, gate[...], preferred_element_type=jnp.float32), clamp_limit
        )
        up_cut = jnp.clip(
            jnp.dot(x, up[...], preferred_element_type=jnp.float32), -clamp_limit, clamp_limit
        )
        active = ((up_cut + 1.0) * (gate_cut * jax.nn.sigmoid(gate_cut * sigmoid_slope))).astype(
            jnp.bfloat16
        )
        tile = min(512, width)
        for start in range(0, width, tile):
            value = scale * jnp.dot(
                active, down[:, start : start + tile], preferred_element_type=jnp.float32
            )
            value = value.astype(jnp.bfloat16)
            for n, (slot, _, _) in enumerate(places):
                part[slot, :, start : start + tile] = value[n * piece_rows : (n + 1) * piece_rows]
        for pair, piece in pairs:
            share(pair, piece).start()

    def settle(h, o, s, entry):
        plane = plane_of(h)
        pair = plane * 2 + column_of(o)
        slot = (pair * 2 + c) * PIECES + s
        rank = (plane * 2 + o) * PIECES + s
        lane = pair * PIECES + s
        row = plane * PIECES + s
        whole, first, second = (
            pl.ds(0, piece_rows), pl.ds(0, piece_rows // 2), pl.ds(piece_rows // 2, piece_rows // 2)
        )
        share(pair, s).wait_recv()
        acc[...] = part[slot].astype(jnp.float32) + cbuf[lane].astype(jnp.float32)

        def upon(side):
            return side * (2 * PLANES * PIECES) + rank

        def climb(side, device, span):
            return remote(
                part.at[slot, span], zbuf.at[upon(side), span],
                sent.at[5], climbed.at[upon(side)], device,
            )

        def over(span):
            return remote(
                part.at[slot, span], ybuf.at[row, span], sent.at[5], crossed.at[row], ypeer
            )

        def take(comes, halved, half, copy, buffer, at):
            for span, wanted in (
                (whole, jnp.logical_and(comes, jnp.logical_not(halved))),
                (half, jnp.logical_and(comes, halved)),
            ):
                @pl.when(wanted)
                def _(span=span):
                    copy(span).wait_recv()
                    acc[span, :] += buffer[at, span, :].astype(jnp.float32)

        halved = (entry >> 13) & 1 == 1
        take((entry >> 8) & 1 == 1, halved, first, over, ybuf, row)
        for bit, side, device in ((9, 1 - flipped, above), (10, flipped, below)):
            take(
                (entry >> bit) & 1 == 1, jnp.logical_and(halved, o == 1), second,
                lambda span, side=side, device=device: climb(side, device, span),
                zbuf, upon(side),
            )

        goal = (entry >> 11) & 3

        @pl.when(goal == 3)
        def _():
            out_ref[pl.ds(pl.multiple_of(s * piece_rows, piece_rows), piece_rows), :] = (
                acc[...].astype(jnp.bfloat16)
            )

        @pl.when(goal != 3)
        def _():
            part[slot] = acc[...].astype(jnp.bfloat16)

        split = (entry >> 14) & 1 == 1
        pl.when(goal == 0)(lambda: over(whole).start())
        pl.when(split)(lambda: over(first).start())
        for way, side, device in ((1, flipped, above), (2, 1 - flipped, below)):
            for span, wanted in ((whole, jnp.logical_not(split)), (second, split)):
                pl.when(jnp.logical_and(goal == way, wanted))(
                    lambda side=side, device=device, span=span: climb(side, device, span).start()
                )

    groups = max(len(END_WORDS), len(MID_WORDS)) // (GROUP // 2)

    def group_step(g, _):
        words = []
        for n in range(GROUP // 2):
            word = jnp.where(is_end, END_WORDS[n], MID_WORDS[n])
            for k in range(1, groups):
                at = k * (GROUP // 2) + n
                word = jnp.where(g == k, jnp.where(is_end, END_WORDS[at], MID_WORDS[at]), word)
            words.append(word)

        def entry_step(j, _):
            word = words[0]
            for n in range(1, GROUP // 2):
                word = jnp.where(j // 2 == n, words[n], word)
            entry = jnp.where(j % 2 == 0, word & 32767, word >> 15)
            kind = entry & 7
            h, o, s = (entry >> 3) & 3, (entry >> 5) & 1, (entry >> 6) & 3
            pl.when(kind == RELAY)(lambda: relay(h, o, s, entry))
            pl.when(kind == CROSS)(lambda: cross(h, s))
            pl.when(kind == COMPUTE)(lambda: compute(h, o, s, entry))
            pl.when(kind == SETTLE)(lambda: settle(h, o, s, entry))
            return 0

        lax.fori_loop(0, GROUP, entry_step, 0)
        return 0

    lax.fori_loop(0, groups, group_step, 0)

    def drain(counts, tiles):
        for kind, count in enumerate(counts):
            if count:
                whole = tok.at[pl.ds(0, count)]
                pltpu.make_async_copy(whole, whole, sent.at[kind]).wait()
        for kind, count in enumerate(tiles):
            if count:
                whole = routes.at[pl.ds(0, count)]
                pltpu.make_async_copy(whole, whole, rsent.at[kind]).wait()

    pl.when(is_end)(lambda: drain(END_SENT, END_TILES))
    pl.when(jnp.logical_not(is_end))(lambda: drain(MID_SENT, MID_TILES))


def dense_body(tokens, norm_gain, expert_ids, route_weight, gate_weight, up_weight, down_weight):
    devices = lax.axis_size("ep")
    rows, width = tokens.shape
    top = expert_ids.shape[1]
    hidden = gate_weight.shape[2]
    piece_rows = rows // PIECES
    vmem, dma = pltpu.VMEM, pltpu.SemaphoreType.DMA
    block = jnp.bfloat16
    lanes = devices // 2 * PIECES
    return pl.pallas_call(
        dense_kernel,
        out_shape=jax.ShapeDtypeStruct((rows, width), block),
        in_specs=[pl.BlockSpec(memory_space=pltpu.HBM)] * 7,
        out_specs=pl.BlockSpec(memory_space=vmem),
        scratch_shapes=[
            vmem((devices * PIECES, piece_rows, width), block),
            vmem((devices * PIECES, piece_rows, width), block),
            vmem((lanes, piece_rows, width), block),
            vmem((PLANES * PIECES, piece_rows, width), block),
            vmem((4 * PLANES * PIECES, piece_rows, width), block),
            vmem((piece_rows, width), jnp.float32),
            vmem((devices, PLANES, rows), jnp.float32),
            vmem((rows, width), block),
            vmem((1, width), jnp.float32),
            vmem((top, rows), jnp.int32),
            vmem((top, rows), jnp.float32),
            vmem((width, hidden), block),
            vmem((width, hidden), block),
            vmem((hidden, width), block),
            dma((6,)),
            dma((PIECES,)),
            dma((devices * PIECES,)),
            dma((devices,)),
            dma((lanes,)),
            dma((PLANES * PIECES,)),
            dma((4 * PLANES * PIECES,)),
            dma((6,)),
            dma((4,)),
        ],
        compiler_params=pltpu.CompilerParams(
            collective_id=0, has_side_effects=True, vmem_limit_bytes=40 * 1024 * 1024
        ),
        name="dense_experts",
    )(
        *[
            pltpu.with_memory_space_constraint(array, pltpu.HBM)
            for array in (
                tokens, norm_gain.reshape(1, width), expert_ids.T, route_weight.T,
                gate_weight, up_weight, down_weight,
            )
        ]
    )


def body(tokens, norm_gain, expert_ids, route_weight, gate_weight, up_weight, down_weight):
    tok_rows, top_count = expert_ids.shape
    experts = lax.axis_size("ep") // SPLIT
    capacity = min(tok_rows, 2 * tok_rows * top_count // experts)
    dense = capacity == tok_rows and experts == PLANES and tok_rows % (32 * PIECES) == 0
    chosen = dense_body if dense else slot_body
    return chosen(
        tokens, norm_gain, expert_ids, route_weight, gate_weight, up_weight, down_weight
    )


def solution(mesh):
    placed = (
        P(("grp", "ep"), None),
        P(),
        P(("grp", "ep"), None),
        P(("grp", "ep"), None),
        P("ep", None, None),
        P("ep", None, None),
        P("ep", None, None),
    )
    return jax.shard_map(
        body, mesh=mesh, in_specs=placed, out_specs=P(("grp", "ep"), None), check_vma=False
    )
```

```python
import functools

import jax
import jax.numpy as jnp
from jax import lax
from jax.experimental import pallas as pl
from jax.experimental.pallas import tpu as pltpu
from jax.sharding import PartitionSpec as P

SPLIT = 4


EPSILON = 1e-05
clamp_limit = 7.0
sigmoid_slope = 1.702


def swapped(array, axis, bit):
    return lax.ppermute(array, axis, [(i, i ^ 1 << bit) for i in range(lax.axis_size(axis))])


def layer_norm(tokens, norm_gain):
    values = tokens.astype(jnp.float32)
    center = values - jnp.mean(values, axis=-1, keepdims=True)
    spread = jnp.mean(center * center, axis=-1, keepdims=True)
    return (center * lax.rsqrt(spread + EPSILON) * norm_gain).astype(jnp.bfloat16)


def expert_rows(block_rows, gate_weight, up_weight, down_weight):
    gate_pre = jnp.einsum(
        "scd,df->scf", block_rows, gate_weight[0], preferred_element_type=jnp.float32
    )
    up_pre = jnp.einsum("scd,df->scf", block_rows, up_weight[0], preferred_element_type=jnp.float32)
    gate_cut = jnp.minimum(gate_pre, clamp_limit)
    up_cut = jnp.clip(up_pre, -clamp_limit, clamp_limit)
    active = ((up_cut + 1.0) * (gate_cut * jax.nn.sigmoid(gate_cut * sigmoid_slope))).astype(
        jnp.bfloat16
    )
    return jnp.einsum("scf,fd->scd", active, down_weight[0], preferred_element_type=jnp.float32)


def slot_body(tokens, norm_gain, expert_ids, route_weight, gate_weight, up_weight, down_weight):
    normed = layer_norm(tokens, norm_gain)
    devices = lax.axis_size("ep")
    experts = devices // SPLIT
    tok_rows = tokens.shape[0]
    top_count = expert_ids.shape[1]
    width = tokens.shape[1]
    capacity = min(tok_rows, 2 * tok_rows * top_count // experts)
    quarter = capacity // SPLIT
    levels = SPLIT.bit_length() - 1
    position = lax.axis_index("ep")
    flat_ids = expert_ids.reshape(-1)
    onehot = (flat_ids[:, None] == jnp.arange(experts, dtype=jnp.int32)[None, :]).astype(jnp.int32)
    earlier = jnp.cumsum(onehot, axis=0) - onehot
    slot_index = jnp.sum(earlier * onehot, axis=1)
    target = flat_ids * capacity + slot_index
    owners = jnp.arange(flat_ids.shape[0], dtype=jnp.int32) // top_count
    slot_token = jnp.full((experts * capacity,), tok_rows, jnp.int32).at[target].set(owners)
    padded = jnp.concatenate([normed, jnp.zeros((1, width), jnp.bfloat16)], axis=0)
    outgoing = jnp.take(padded, slot_token, axis=0).reshape(experts, capacity, width)
    pieces = outgoing.reshape(devices, quarter, width)
    gathered = lax.all_to_all(pieces, "ep", split_axis=0, concat_axis=0, tiled=True)
    for bit_level in range(levels):
        partner = swapped(gathered, "ep", bit_level)
        upper_bit = position >> bit_level & 1
        first_half = jnp.where(upper_bit == 1, partner, gathered)
        second_half = jnp.where(upper_bit == 1, gathered, partner)
        gathered = jnp.concatenate([first_half, second_half], axis=1)
    partial_value = expert_rows(gathered, gate_weight, up_weight, down_weight)
    length = capacity
    for bit_level in reversed(range(levels)):
        length = length // 2
        upper_bit = position >> bit_level & 1
        kept_rows = lax.dynamic_slice_in_dim(partial_value, upper_bit * length, length, 1)
        sent_rows = lax.dynamic_slice_in_dim(partial_value, (1 - upper_bit) * length, length, 1)
        partial_value = kept_rows + swapped(sent_rows, "ep", bit_level)
    finished = partial_value.astype(jnp.bfloat16)
    returned = lax.all_to_all(finished, "ep", split_axis=0, concat_axis=0, tiled=True)
    results = returned.reshape(experts * capacity, width)
    picked = jnp.take(results, target, axis=0).reshape(tok_rows, top_count, width)
    combined = jnp.sum(route_weight[:, :, None] * picked.astype(jnp.float32), axis=1)
    return combined.astype(jnp.bfloat16)


MESH = pl.DeviceIdType.MESH
PLANES = 4
PIECES = 4

RELAY, CROSS, COMPUTE, SETTLE = 0, 1, 2, 3
GROUP = 8
END_WORDS = (
    262337, 4227081, 2392136, 15728672, 1335306, 4458507,
    345309321, 524488, 68517905, 69566568, 4732946, 573898897,
    788499, 1572889, 5509858, 2885739, 832110681, 6817939,
    1835217, 1147056, 68785498, 8126624, 3932225, 6047666,
    7866459, 72978426, 257753147, 8224880, 7080059, 611942587,
    4980832, 76389330, 5608306, 7604699, 80576592, 108331123,
    350851410, 211886819, 78217451, 172034443, 22119011, 226593227,
    232889155, 138115,
)
MID_WORDS = (
    8388681, 1310721, 4497866, 847315472, 557376, 1048960,
    21495937, 819736, 15728705, 411631664, 856752728, 4751776,
    11796648, 14680265, 296551120, 2916408, 239665912, 5767864,
    530385939, 20447441, 8227138, 21758680, 3146472, 105480251,
    1147000, 190644816, 163384371, 120672483, 231803995, 51743923,
    6127731, 182518000, 139562107, 255922755, 260410651, 309960018,
    154242523, 221577899, 159485339, 115967083, 7713731, 155290963,
    262512523, 139211,
)
END_SENT = (12, 5, 0, 32, 32, 28)
END_TILES = (4, 1, 0, 8)
MID_SENT = (12, 11, 16, 32, 32, 28)
MID_TILES = (4, 2, 3, 8)


def lane_column(row, piece, rows):
    lanes = lax.broadcasted_iota(jnp.int32, (rows, row.shape[1]), 1)
    line = lax.broadcasted_iota(jnp.int32, (rows, row.shape[1]), 0)
    return jnp.sum(jnp.where(lanes == piece * rows + line, row, 0.0), axis=1, keepdims=True)


def dense_kernel(
    tokens_hbm, gain_hbm, ids_hbm, route_hbm, gate_hbm, up_hbm, down_hbm,
    out_ref,
    tok, part, cbuf, ybuf, zbuf, acc, routes, tokens, gain, ids, route, gate, up, down,
    lsem, wsem, arrived, routed, shared, crossed, climbed, sent, rsent,
):
    rows, width = tokens_hbm.shape
    piece_rows = rows // PIECES
    me = lax.axis_index("ep")
    z, y, c = me // 4, (me // 2) % 2, me % 2
    flipped = (z >= PLANES // 2).astype(jnp.int32)
    level = jnp.where(z >= PLANES // 2, PLANES - 1 - z, z)
    is_end = level == 0
    upward = 1 - 2 * flipped
    ypeer, cpeer = z * 4 + (1 - y) * 2 + c, z * 4 + y * 2 + 1 - c
    above, below = me + 4 * upward, me - 4 * upward

    def plane_of(h):
        return jnp.where(z >= PLANES // 2, PLANES - 1 - h, h)

    def column_of(o):
        return jnp.where(o == 0, y, 1 - y)

    def remote(source, target, send_sem, recv_sem, device):
        return pltpu.make_async_remote_copy(
            src_ref=source, dst_ref=target, send_sem=send_sem, recv_sem=recv_sem,
            device_id={"ep": device}, device_id_type=MESH,
        )

    def move(kind, slot, device):
        return remote(tok.at[slot], tok.at[slot], sent.at[kind], arrived.at[slot], device)

    def move_route(kind, block, device):
        return remote(
            routes.at[block], routes.at[block], rsent.at[kind], routed.at[block], device
        )

    def hand(kind, slot, block, first, device):
        move(kind, slot, device).start()
        pl.when(first)(lambda: move_route(kind, block, device).start())

    barrier = pltpu.get_barrier_semaphore()

    def greet(device):
        pl.semaphore_signal(barrier, inc=1, device_id={"ep": device}, device_id_type=MESH)

    greet(ypeer)
    greet(cpeer)
    greet(above)
    pl.when(jnp.logical_not(is_end))(lambda: greet(below))

    def load_piece(s):
        span = pl.ds(pl.multiple_of(s * piece_rows, piece_rows), piece_rows)
        return pltpu.make_async_copy(tokens_hbm.at[span], tokens.at[span], wsem.at[s])

    small_loads = [
        pltpu.make_async_copy(ids_hbm, ids, lsem.at[0]),
        pltpu.make_async_copy(route_hbm, route, lsem.at[1]),
        pltpu.make_async_copy(gain_hbm, gain, lsem.at[2]),
    ]
    weight_loads = [
        pltpu.make_async_copy(gate_hbm.at[0], gate, lsem.at[3]),
        pltpu.make_async_copy(up_hbm.at[0], up, lsem.at[4]),
        pltpu.make_async_copy(down_hbm.at[0], down, lsem.at[5]),
    ]
    for s in range(PIECES):
        load_piece(s).start()
    for load in small_loads + weight_loads:
        load.start()

    for load in small_loads:
        load.wait()
    for e in range(PLANES):
        routes[me, e : e + 1, :] = jnp.sum(
            jnp.where(ids[...] == e, route[...], 0.0), axis=0, keepdims=True
        )

    def open_step(s, _):
        span = pl.ds(pl.multiple_of(s * piece_rows, piece_rows), piece_rows)
        load_piece(s).wait()
        values = tokens[span, :].astype(jnp.float32)
        center = values - jnp.mean(values, axis=-1, keepdims=True)
        spread = jnp.mean(center * center, axis=-1, keepdims=True)
        slot = me * PIECES + s
        tok[slot] = (center * lax.rsqrt(spread + EPSILON) * gain[...]).astype(jnp.bfloat16)

        @pl.when(s == 0)
        def _():
            pl.semaphore_wait(barrier, jnp.where(is_end, 3, 4))

        hand(1, slot, me, s == 0, above)
        pl.when(jnp.logical_not(is_end))(lambda: hand(2, slot, me, s == 0, below))
        pl.when(s == 0)(lambda: hand(0, slot, me, True, ypeer))
        hand(3, slot, me, s == 0, cpeer)
        return 0

    lax.fori_loop(0, PIECES, open_step, 0)
    for load in weight_loads:
        load.wait()

    def relay(h, o, s, entry):
        block = plane_of(h) * 4 + column_of(o) * 2 + c
        slot = block * PIECES + s
        move(3, slot, cpeer).wait_recv()
        pl.when(s == 0)(lambda: move_route(3, block, cpeer).wait_recv())
        pl.when((entry >> 8) & 1 == 1)(lambda: hand(1, slot, block, s == 0, above))
        pl.when((entry >> 9) & 1 == 1)(lambda: hand(2, slot, block, s == 0, below))
        hand(3, slot, block, s == 0, cpeer)

    def cross(h, s):
        block = plane_of(h) * 4 + y * 2 + c
        hand(0, block * PIECES + s, block, s == 0, ypeer)

    def share(pair, s):
        return remote(
            part.at[(pair * 2 + 1 - c) * PIECES + s], cbuf.at[pair * PIECES + s],
            sent.at[4], shared.at[pair * PIECES + s], cpeer,
        )

    def compute(h, o, s, entry):
        h2, o2, s2 = (entry >> 8) & 3, (entry >> 10) & 1, (entry >> 11) & 3
        pairs = [(plane_of(h) * 2 + column_of(o), s), (plane_of(h2) * 2 + column_of(o2), s2)]
        for n, (pair, piece) in enumerate(pairs):
            block = pair * 2 + 1 - c
            move(3, block * PIECES + piece, cpeer).wait_recv()
            pl.when((entry >> (13 + n)) & 1 == 1)(
                lambda block=block: move_route(3, block, cpeer).wait_recv()
            )
        places = [
            ((pair * 2 + core) * PIECES + piece, pair * 2 + core, piece)
            for pair, piece in pairs
            for core in range(2)
        ]
        x = jnp.concatenate([tok[slot] for slot, _, _ in places], axis=0)
        scale = jnp.concatenate(
            [
                lane_column(routes[block, pl.ds(z, 1), :], piece, piece_rows)
                for _, block, piece in places
            ],
            axis=0,
        )
        gate_cut = jnp.minimum(
            jnp.dot(x, gate[...], preferred_element_type=jnp.float32), clamp_limit
        )
        up_cut = jnp.clip(
            jnp.dot(x, up[...], preferred_element_type=jnp.float32), -clamp_limit, clamp_limit
        )
        active = ((up_cut + 1.0) * (gate_cut * jax.nn.sigmoid(gate_cut * sigmoid_slope))).astype(
            jnp.bfloat16
        )
        tile = min(512, width)
        for start in range(0, width, tile):
            value = scale * jnp.dot(
                active, down[:, start : start + tile], preferred_element_type=jnp.float32
            )
            value = value.astype(jnp.bfloat16)
            for n, (slot, _, _) in enumerate(places):
                part[slot, :, start : start + tile] = value[n * piece_rows : (n + 1) * piece_rows]
        for pair, piece in pairs:
            share(pair, piece).start()

    def settle(h, o, s, entry):
        plane = plane_of(h)
        pair = plane * 2 + column_of(o)
        slot = (pair * 2 + c) * PIECES + s
        rank = (plane * 2 + o) * PIECES + s
        lane = pair * PIECES + s
        row = plane * PIECES + s
        whole, first, second = (
            pl.ds(0, piece_rows), pl.ds(0, piece_rows // 2), pl.ds(piece_rows // 2, piece_rows // 2)
        )
        share(pair, s).wait_recv()
        acc[...] = part[slot].astype(jnp.float32) + cbuf[lane].astype(jnp.float32)

        def upon(side):
            return side * (2 * PLANES * PIECES) + rank

        def climb(side, device, span):
            return remote(
                part.at[slot, span], zbuf.at[upon(side), span],
                sent.at[5], climbed.at[upon(side)], device,
            )

        def over(span):
            return remote(
                part.at[slot, span], ybuf.at[row, span], sent.at[5], crossed.at[row], ypeer
            )

        def take(comes, halved, half, copy, buffer, at):
            for span, wanted in (
                (whole, jnp.logical_and(comes, jnp.logical_not(halved))),
                (half, jnp.logical_and(comes, halved)),
            ):
                @pl.when(wanted)
                def _(span=span):
                    copy(span).wait_recv()
                    acc[span, :] += buffer[at, span, :].astype(jnp.float32)

        halved = (entry >> 13) & 1 == 1
        take((entry >> 8) & 1 == 1, halved, first, over, ybuf, row)
        for bit, side, device in ((9, 1 - flipped, above), (10, flipped, below)):
            take(
                (entry >> bit) & 1 == 1, jnp.logical_and(halved, o == 1), second,
                lambda span, side=side, device=device: climb(side, device, span),
                zbuf, upon(side),
            )

        goal = (entry >> 11) & 3

        @pl.when(goal == 3)
        def _():
            out_ref[pl.ds(pl.multiple_of(s * piece_rows, piece_rows), piece_rows), :] = (
                acc[...].astype(jnp.bfloat16)
            )

        @pl.when(goal != 3)
        def _():
            part[slot] = acc[...].astype(jnp.bfloat16)

        split = (entry >> 14) & 1 == 1
        pl.when(goal == 0)(lambda: over(whole).start())
        pl.when(split)(lambda: over(first).start())
        for way, side, device in ((1, flipped, above), (2, 1 - flipped, below)):
            for span, wanted in ((whole, jnp.logical_not(split)), (second, split)):
                pl.when(jnp.logical_and(goal == way, wanted))(
                    lambda side=side, device=device, span=span: climb(side, device, span).start()
                )

    groups = max(len(END_WORDS), len(MID_WORDS)) // (GROUP // 2)

    def group_step(g, _):
        words = []
        for n in range(GROUP // 2):
            word = jnp.where(is_end, END_WORDS[n], MID_WORDS[n])
            for k in range(1, groups):
                at = k * (GROUP // 2) + n
                word = jnp.where(g == k, jnp.where(is_end, END_WORDS[at], MID_WORDS[at]), word)
            words.append(word)

        def entry_step(j, _):
            word = words[0]
            for n in range(1, GROUP // 2):
                word = jnp.where(j // 2 == n, words[n], word)
            entry = jnp.where(j % 2 == 0, word & 32767, word >> 15)
            kind = entry & 7
            h, o, s = (entry >> 3) & 3, (entry >> 5) & 1, (entry >> 6) & 3
            pl.when(kind == RELAY)(lambda: relay(h, o, s, entry))
            pl.when(kind == CROSS)(lambda: cross(h, s))
            pl.when(kind == COMPUTE)(lambda: compute(h, o, s, entry))
            pl.when(kind == SETTLE)(lambda: settle(h, o, s, entry))
            return 0

        lax.fori_loop(0, GROUP, entry_step, 0)
        return 0

    lax.fori_loop(0, groups, group_step, 0)

    def drain(counts, tiles):
        for kind, count in enumerate(counts):
            if count:
                whole = tok.at[pl.ds(0, count)]
                pltpu.make_async_copy(whole, whole, sent.at[kind]).wait()
        for kind, count in enumerate(tiles):
            if count:
                whole = routes.at[pl.ds(0, count)]
                pltpu.make_async_copy(whole, whole, rsent.at[kind]).wait()

    pl.when(is_end)(lambda: drain(END_SENT, END_TILES))
    pl.when(jnp.logical_not(is_end))(lambda: drain(MID_SENT, MID_TILES))


def dense_body(tokens, norm_gain, expert_ids, route_weight, gate_weight, up_weight, down_weight):
    devices = lax.axis_size("ep")
    rows, width = tokens.shape
    top = expert_ids.shape[1]
    hidden = gate_weight.shape[2]
    piece_rows = rows // PIECES
    vmem, dma = pltpu.VMEM, pltpu.SemaphoreType.DMA
    block = jnp.bfloat16
    lanes = devices // 2 * PIECES
    return pl.pallas_call(
        dense_kernel,
        out_shape=jax.ShapeDtypeStruct((rows, width), block),
        in_specs=[pl.BlockSpec(memory_space=pltpu.HBM)] * 7,
        out_specs=pl.BlockSpec(memory_space=vmem),
        scratch_shapes=[
            vmem((devices * PIECES, piece_rows, width), block),
            vmem((devices * PIECES, piece_rows, width), block),
            vmem((lanes, piece_rows, width), block),
            vmem((PLANES * PIECES, piece_rows, width), block),
            vmem((4 * PLANES * PIECES, piece_rows, width), block),
            vmem((piece_rows, width), jnp.float32),
            vmem((devices, PLANES, rows), jnp.float32),
            vmem((rows, width), block),
            vmem((1, width), jnp.float32),
            vmem((top, rows), jnp.int32),
            vmem((top, rows), jnp.float32),
            vmem((width, hidden), block),
            vmem((width, hidden), block),
            vmem((hidden, width), block),
            dma((6,)),
            dma((PIECES,)),
            dma((devices * PIECES,)),
            dma((devices,)),
            dma((lanes,)),
            dma((PLANES * PIECES,)),
            dma((4 * PLANES * PIECES,)),
            dma((6,)),
            dma((4,)),
        ],
        compiler_params=pltpu.CompilerParams(
            collective_id=0, has_side_effects=True, vmem_limit_bytes=40 * 1024 * 1024
        ),
        name="dense_experts",
    )(
        *[
            pltpu.with_memory_space_constraint(array, pltpu.HBM)
            for array in (
                tokens, norm_gain.reshape(1, width), expert_ids.T, route_weight.T,
                gate_weight, up_weight, down_weight,
            )
        ]
    )


def body(tokens, norm_gain, expert_ids, route_weight, gate_weight, up_weight, down_weight):
    tok_rows, top_count = expert_ids.shape
    experts = lax.axis_size("ep") // SPLIT
    capacity = min(tok_rows, 2 * tok_rows * top_count // experts)
    dense = capacity == tok_rows and experts == PLANES and tok_rows % (32 * PIECES) == 0
    chosen = dense_body if dense else slot_body
    return chosen(
        tokens, norm_gain, expert_ids, route_weight, gate_weight, up_weight, down_weight
    )


def solution(mesh):
    placed = (
        P(("grp", "ep"), None),
        P(),
        P(("grp", "ep"), None),
        P(("grp", "ep"), None),
        P("ep", None, None),
        P("ep", None, None),
        P("ep", None, None),
    )
    return jax.shard_map(
        body, mesh=mesh, in_specs=placed, out_specs=P(("grp", "ep"), None), check_vma=False
    )
```

```python
import functools

import jax
import jax.numpy as jnp
from jax import lax
from jax.experimental import pallas as pl
from jax.experimental.pallas import tpu as pltpu
from jax.sharding import PartitionSpec as P

SPLIT = 4


EPSILON = 1e-05
clamp_limit = 7.0
sigmoid_slope = 1.702


def swapped(array, axis, bit):
    return lax.ppermute(array, axis, [(i, i ^ 1 << bit) for i in range(lax.axis_size(axis))])


def layer_norm(tokens, norm_gain):
    values = tokens.astype(jnp.float32)
    center = values - jnp.mean(values, axis=-1, keepdims=True)
    spread = jnp.mean(center * center, axis=-1, keepdims=True)
    return (center * lax.rsqrt(spread + EPSILON) * norm_gain).astype(jnp.bfloat16)


def expert_rows(block_rows, gate_weight, up_weight, down_weight):
    gate_pre = jnp.einsum(
        "scd,df->scf", block_rows, gate_weight[0], preferred_element_type=jnp.float32
    )
    up_pre = jnp.einsum("scd,df->scf", block_rows, up_weight[0], preferred_element_type=jnp.float32)
    gate_cut = jnp.minimum(gate_pre, clamp_limit)
    up_cut = jnp.clip(up_pre, -clamp_limit, clamp_limit)
    active = ((up_cut + 1.0) * (gate_cut * jax.nn.sigmoid(gate_cut * sigmoid_slope))).astype(
        jnp.bfloat16
    )
    return jnp.einsum("scf,fd->scd", active, down_weight[0], preferred_element_type=jnp.float32)


def slot_body(tokens, norm_gain, expert_ids, route_weight, gate_weight, up_weight, down_weight):
    normed = layer_norm(tokens, norm_gain)
    devices = lax.axis_size("ep")
    experts = devices // SPLIT
    tok_rows = tokens.shape[0]
    top_count = expert_ids.shape[1]
    width = tokens.shape[1]
    capacity = min(tok_rows, 2 * tok_rows * top_count // experts)
    quarter = capacity // SPLIT
    levels = SPLIT.bit_length() - 1
    position = lax.axis_index("ep")
    flat_ids = expert_ids.reshape(-1)
    onehot = (flat_ids[:, None] == jnp.arange(experts, dtype=jnp.int32)[None, :]).astype(jnp.int32)
    earlier = jnp.cumsum(onehot, axis=0) - onehot
    slot_index = jnp.sum(earlier * onehot, axis=1)
    target = flat_ids * capacity + slot_index
    owners = jnp.arange(flat_ids.shape[0], dtype=jnp.int32) // top_count
    slot_token = jnp.full((experts * capacity,), tok_rows, jnp.int32).at[target].set(owners)
    padded = jnp.concatenate([normed, jnp.zeros((1, width), jnp.bfloat16)], axis=0)
    outgoing = jnp.take(padded, slot_token, axis=0).reshape(experts, capacity, width)
    pieces = outgoing.reshape(devices, quarter, width)
    gathered = lax.all_to_all(pieces, "ep", split_axis=0, concat_axis=0, tiled=True)
    for bit_level in range(levels):
        partner = swapped(gathered, "ep", bit_level)
        upper_bit = position >> bit_level & 1
        first_half = jnp.where(upper_bit == 1, partner, gathered)
        second_half = jnp.where(upper_bit == 1, gathered, partner)
        gathered = jnp.concatenate([first_half, second_half], axis=1)
    partial_value = expert_rows(gathered, gate_weight, up_weight, down_weight)
    length = capacity
    for bit_level in reversed(range(levels)):
        length = length // 2
        upper_bit = position >> bit_level & 1
        kept_rows = lax.dynamic_slice_in_dim(partial_value, upper_bit * length, length, 1)
        sent_rows = lax.dynamic_slice_in_dim(partial_value, (1 - upper_bit) * length, length, 1)
        partial_value = kept_rows + swapped(sent_rows, "ep", bit_level)
    finished = partial_value.astype(jnp.bfloat16)
    returned = lax.all_to_all(finished, "ep", split_axis=0, concat_axis=0, tiled=True)
    results = returned.reshape(experts * capacity, width)
    picked = jnp.take(results, target, axis=0).reshape(tok_rows, top_count, width)
    combined = jnp.sum(route_weight[:, :, None] * picked.astype(jnp.float32), axis=1)
    return combined.astype(jnp.bfloat16)


MESH = pl.DeviceIdType.MESH
PLANES = 4
PIECES = 4

RELAY, CROSS, COMPUTE, SETTLE = 0, 1, 2, 3
GROUP = 8
END_WORDS = (
    262337, 4227081, 2384130, 1048649, 15728680, 203753483,
    848363585, 557072, 69566568, 2623531, 557121617, 819224,
    4456496, 237570155, 4982803, 3670169, 1847602, 2916440,
    6555731, 68780233, 6041146, 5514074, 70877243, 3932408,
    1151930, 7866459, 6131706, 5245211, 184090840, 7604347,
    5767419, 7969698, 5605787, 249102544, 82673808, 5867730,
    7438432, 155257067, 82412195, 80320866, 226592971, 20023691,
    228694915, 138179,
)
MID_WORDS = (
    6586505, 8401162, 2392065, 1311248, 12583504, 847315264,
    4227560, 17563680, 15728657, 839450728, 819864, 13635810,
    2654808, 1573312, 2130856, 336396515, 379125816, 24903792,
    24659802, 6029347, 174392427, 1933664, 101286616, 22550466,
    102342514, 23597922, 37322939, 3932816, 103651058, 139565690,
    8228123, 153193595, 91031083, 159485339, 183828723, 116232803,
    260407475, 155290963, 41255083, 115970634, 113873859, 266706763,
    139147, 131076,
)
END_SENT = (12, 5, 0, 32, 32, 28)
END_TILES = (4, 1, 0, 8)
MID_SENT = (10, 13, 16, 32, 32, 28)
MID_TILES = (4, 2, 3, 8)


def lane_column(row, piece, rows):
    lanes = lax.broadcasted_iota(jnp.int32, (rows, row.shape[1]), 1)
    line = lax.broadcasted_iota(jnp.int32, (rows, row.shape[1]), 0)
    return jnp.sum(jnp.where(lanes == piece * rows + line, row, 0.0), axis=1, keepdims=True)


def dense_kernel(
    tokens_hbm, gain_hbm, ids_hbm, route_hbm, gate_hbm, up_hbm, down_hbm,
    out_ref,
    tok, part, cbuf, ybuf, zbuf, acc, routes, tokens, gain, ids, route, gate, up, down,
    lsem, wsem, arrived, routed, shared, crossed, climbed, sent, rsent,
):
    rows, width = tokens_hbm.shape
    piece_rows = rows // PIECES
    me = lax.axis_index("ep")
    z, y, c = me // 4, (me // 2) % 2, me % 2
    flipped = (z >= PLANES // 2).astype(jnp.int32)
    level = jnp.where(z >= PLANES // 2, PLANES - 1 - z, z)
    is_end = level == 0
    upward = 1 - 2 * flipped
    ypeer, cpeer = z * 4 + (1 - y) * 2 + c, z * 4 + y * 2 + 1 - c
    above, below = me + 4 * upward, me - 4 * upward

    def plane_of(h):
        return jnp.where(z >= PLANES // 2, PLANES - 1 - h, h)

    def column_of(o):
        return jnp.where(o == 0, y, 1 - y)

    def remote(source, target, send_sem, recv_sem, device):
        return pltpu.make_async_remote_copy(
            src_ref=source, dst_ref=target, send_sem=send_sem, recv_sem=recv_sem,
            device_id={"ep": device}, device_id_type=MESH,
        )

    def move(kind, slot, device):
        return remote(tok.at[slot], tok.at[slot], sent.at[kind], arrived.at[slot], device)

    def move_route(kind, block, device):
        return remote(
            routes.at[block], routes.at[block], rsent.at[kind], routed.at[block], device
        )

    def hand(kind, slot, block, first, device):
        move(kind, slot, device).start()
        pl.when(first)(lambda: move_route(kind, block, device).start())

    barrier = pltpu.get_barrier_semaphore()

    def greet(device):
        pl.semaphore_signal(barrier, inc=1, device_id={"ep": device}, device_id_type=MESH)

    greet(ypeer)
    greet(cpeer)
    greet(above)
    pl.when(jnp.logical_not(is_end))(lambda: greet(below))

    def load_piece(s):
        span = pl.ds(pl.multiple_of(s * piece_rows, piece_rows), piece_rows)
        return pltpu.make_async_copy(tokens_hbm.at[span], tokens.at[span], wsem.at[s])

    small_loads = [
        pltpu.make_async_copy(ids_hbm, ids, lsem.at[0]),
        pltpu.make_async_copy(route_hbm, route, lsem.at[1]),
        pltpu.make_async_copy(gain_hbm, gain, lsem.at[2]),
    ]
    weight_loads = [
        pltpu.make_async_copy(gate_hbm.at[0], gate, lsem.at[3]),
        pltpu.make_async_copy(up_hbm.at[0], up, lsem.at[4]),
        pltpu.make_async_copy(down_hbm.at[0], down, lsem.at[5]),
    ]
    for s in range(PIECES):
        load_piece(s).start()
    for load in small_loads + weight_loads:
        load.start()

    for load in small_loads:
        load.wait()
    for e in range(PLANES):
        routes[me, e : e + 1, :] = jnp.sum(
            jnp.where(ids[...] == e, route[...], 0.0), axis=0, keepdims=True
        )

    def open_step(s, _):
        span = pl.ds(pl.multiple_of(s * piece_rows, piece_rows), piece_rows)
        load_piece(s).wait()
        values = tokens[span, :].astype(jnp.float32)
        center = values - jnp.mean(values, axis=-1, keepdims=True)
        spread = jnp.mean(center * center, axis=-1, keepdims=True)
        slot = me * PIECES + s
        tok[slot] = (center * lax.rsqrt(spread + EPSILON) * gain[...]).astype(jnp.bfloat16)

        @pl.when(s == 0)
        def _():
            pl.semaphore_wait(barrier, jnp.where(is_end, 3, 4))

        hand(1, slot, me, s == 0, above)
        pl.when(jnp.logical_not(is_end))(lambda: hand(2, slot, me, s == 0, below))
        pl.when(s == 0)(lambda: hand(0, slot, me, True, ypeer))
        hand(3, slot, me, s == 0, cpeer)
        return 0

    lax.fori_loop(0, PIECES, open_step, 0)
    for load in weight_loads:
        load.wait()

    def relay(h, o, s, entry):
        block = plane_of(h) * 4 + column_of(o) * 2 + c
        slot = block * PIECES + s
        move(3, slot, cpeer).wait_recv()
        pl.when(s == 0)(lambda: move_route(3, block, cpeer).wait_recv())
        pl.when((entry >> 8) & 1 == 1)(lambda: hand(1, slot, block, s == 0, above))
        pl.when((entry >> 9) & 1 == 1)(lambda: hand(2, slot, block, s == 0, below))
        hand(3, slot, block, s == 0, cpeer)

    def cross(h, s):
        block = plane_of(h) * 4 + y * 2 + c
        hand(0, block * PIECES + s, block, s == 0, ypeer)

    def share(pair, s):
        return remote(
            part.at[(pair * 2 + 1 - c) * PIECES + s], cbuf.at[pair * PIECES + s],
            sent.at[4], shared.at[pair * PIECES + s], cpeer,
        )

    def compute(h, o, s, entry):
        h2, o2, s2 = (entry >> 8) & 3, (entry >> 10) & 1, (entry >> 11) & 3
        pairs = [(plane_of(h) * 2 + column_of(o), s), (plane_of(h2) * 2 + column_of(o2), s2)]
        for n, (pair, piece) in enumerate(pairs):
            block = pair * 2 + 1 - c
            move(3, block * PIECES + piece, cpeer).wait_recv()
            pl.when((entry >> (13 + n)) & 1 == 1)(
                lambda block=block: move_route(3, block, cpeer).wait_recv()
            )
        places = [
            ((pair * 2 + core) * PIECES + piece, pair * 2 + core, piece)
            for pair, piece in pairs
            for core in range(2)
        ]
        x = jnp.concatenate([tok[slot] for slot, _, _ in places], axis=0)
        scale = jnp.concatenate(
            [
                lane_column(routes[block, pl.ds(z, 1), :], piece, piece_rows)
                for _, block, piece in places
            ],
            axis=0,
        )
        gate_cut = jnp.minimum(
            jnp.dot(x, gate[...], preferred_element_type=jnp.float32), clamp_limit
        )
        up_cut = jnp.clip(
            jnp.dot(x, up[...], preferred_element_type=jnp.float32), -clamp_limit, clamp_limit
        )
        active = ((up_cut + 1.0) * (gate_cut * jax.nn.sigmoid(gate_cut * sigmoid_slope))).astype(
            jnp.bfloat16
        )
        tile = min(512, width)
        for start in range(0, width, tile):
            value = scale * jnp.dot(
                active, down[:, start : start + tile], preferred_element_type=jnp.float32
            )
            value = value.astype(jnp.bfloat16)
            for n, (slot, _, _) in enumerate(places):
                part[slot, :, start : start + tile] = value[n * piece_rows : (n + 1) * piece_rows]
        for pair, piece in pairs:
            share(pair, piece).start()

    def settle(h, o, s, entry):
        plane = plane_of(h)
        pair = plane * 2 + column_of(o)
        slot = (pair * 2 + c) * PIECES + s
        rank = (plane * 2 + o) * PIECES + s
        lane = pair * PIECES + s
        row = plane * PIECES + s
        whole, first, second = (
            pl.ds(0, piece_rows), pl.ds(0, piece_rows // 2), pl.ds(piece_rows // 2, piece_rows // 2)
        )
        share(pair, s).wait_recv()
        acc[...] = part[slot].astype(jnp.float32) + cbuf[lane].astype(jnp.float32)

        def upon(side):
            return side * (2 * PLANES * PIECES) + rank

        def climb(side, device, span):
            return remote(
                part.at[slot, span], zbuf.at[upon(side), span],
                sent.at[5], climbed.at[upon(side)], device,
            )

        def over(span):
            return remote(
                part.at[slot, span], ybuf.at[row, span], sent.at[5], crossed.at[row], ypeer
            )

        def take(comes, halved, half, copy, buffer, at):
            for span, wanted in (
                (whole, jnp.logical_and(comes, jnp.logical_not(halved))),
                (half, jnp.logical_and(comes, halved)),
            ):
                @pl.when(wanted)
                def _(span=span):
                    copy(span).wait_recv()
                    acc[span, :] += buffer[at, span, :].astype(jnp.float32)

        halved = (entry >> 13) & 1 == 1
        take((entry >> 8) & 1 == 1, halved, first, over, ybuf, row)
        for bit, side, device in ((9, 1 - flipped, above), (10, flipped, below)):
            take(
                (entry >> bit) & 1 == 1, jnp.logical_and(halved, o == 1), second,
                lambda span, side=side, device=device: climb(side, device, span),
                zbuf, upon(side),
            )

        goal = (entry >> 11) & 3

        @pl.when(goal == 3)
        def _():
            out_ref[pl.ds(pl.multiple_of(s * piece_rows, piece_rows), piece_rows), :] = (
                acc[...].astype(jnp.bfloat16)
            )

        @pl.when(goal != 3)
        def _():
            part[slot] = acc[...].astype(jnp.bfloat16)

        split = (entry >> 14) & 1 == 1
        pl.when(goal == 0)(lambda: over(whole).start())
        pl.when(split)(lambda: over(first).start())
        for way, side, device in ((1, flipped, above), (2, 1 - flipped, below)):
            for span, wanted in ((whole, jnp.logical_not(split)), (second, split)):
                pl.when(jnp.logical_and(goal == way, wanted))(
                    lambda side=side, device=device, span=span: climb(side, device, span).start()
                )

    groups = max(len(END_WORDS), len(MID_WORDS)) // (GROUP // 2)

    def group_step(g, _):
        words = []
        for n in range(GROUP // 2):
            word = jnp.where(is_end, END_WORDS[n], MID_WORDS[n])
            for k in range(1, groups):
                at = k * (GROUP // 2) + n
                word = jnp.where(g == k, jnp.where(is_end, END_WORDS[at], MID_WORDS[at]), word)
            words.append(word)

        def entry_step(j, _):
            word = words[0]
            for n in range(1, GROUP // 2):
                word = jnp.where(j // 2 == n, words[n], word)
            entry = jnp.where(j % 2 == 0, word & 32767, word >> 15)
            kind = entry & 7
            h, o, s = (entry >> 3) & 3, (entry >> 5) & 1, (entry >> 6) & 3
            pl.when(kind == RELAY)(lambda: relay(h, o, s, entry))
            pl.when(kind == CROSS)(lambda: cross(h, s))
            pl.when(kind == COMPUTE)(lambda: compute(h, o, s, entry))
            pl.when(kind == SETTLE)(lambda: settle(h, o, s, entry))
            return 0

        lax.fori_loop(0, GROUP, entry_step, 0)
        return 0

    lax.fori_loop(0, groups, group_step, 0)

    def drain(counts, tiles):
        for kind, count in enumerate(counts):
            if count:
                whole = tok.at[pl.ds(0, count)]
                pltpu.make_async_copy(whole, whole, sent.at[kind]).wait()
        for kind, count in enumerate(tiles):
            if count:
                whole = routes.at[pl.ds(0, count)]
                pltpu.make_async_copy(whole, whole, rsent.at[kind]).wait()

    pl.when(is_end)(lambda: drain(END_SENT, END_TILES))
    pl.when(jnp.logical_not(is_end))(lambda: drain(MID_SENT, MID_TILES))


def dense_body(tokens, norm_gain, expert_ids, route_weight, gate_weight, up_weight, down_weight):
    devices = lax.axis_size("ep")
    rows, width = tokens.shape
    top = expert_ids.shape[1]
    hidden = gate_weight.shape[2]
    piece_rows = rows // PIECES
    vmem, dma = pltpu.VMEM, pltpu.SemaphoreType.DMA
    block = jnp.bfloat16
    lanes = devices // 2 * PIECES
    return pl.pallas_call(
        dense_kernel,
        out_shape=jax.ShapeDtypeStruct((rows, width), block),
        in_specs=[pl.BlockSpec(memory_space=pltpu.HBM)] * 7,
        out_specs=pl.BlockSpec(memory_space=vmem),
        scratch_shapes=[
            vmem((devices * PIECES, piece_rows, width), block),
            vmem((devices * PIECES, piece_rows, width), block),
            vmem((lanes, piece_rows, width), block),
            vmem((PLANES * PIECES, piece_rows, width), block),
            vmem((4 * PLANES * PIECES, piece_rows, width), block),
            vmem((piece_rows, width), jnp.float32),
            vmem((devices, PLANES, rows), jnp.float32),
            vmem((rows, width), block),
            vmem((1, width), jnp.float32),
            vmem((top, rows), jnp.int32),
            vmem((top, rows), jnp.float32),
            vmem((width, hidden), block),
            vmem((width, hidden), block),
            vmem((hidden, width), block),
            dma((6,)),
            dma((PIECES,)),
            dma((devices * PIECES,)),
            dma((devices,)),
            dma((lanes,)),
            dma((PLANES * PIECES,)),
            dma((4 * PLANES * PIECES,)),
            dma((6,)),
            dma((4,)),
        ],
        compiler_params=pltpu.CompilerParams(
            collective_id=0, has_side_effects=True, vmem_limit_bytes=40 * 1024 * 1024
        ),
        name="dense_experts",
    )(
        *[
            pltpu.with_memory_space_constraint(array, pltpu.HBM)
            for array in (
                tokens, norm_gain.reshape(1, width), expert_ids.T, route_weight.T,
                gate_weight, up_weight, down_weight,
            )
        ]
    )


def body(tokens, norm_gain, expert_ids, route_weight, gate_weight, up_weight, down_weight):
    tok_rows, top_count = expert_ids.shape
    experts = lax.axis_size("ep") // SPLIT
    capacity = min(tok_rows, 2 * tok_rows * top_count // experts)
    dense = capacity == tok_rows and experts == PLANES and tok_rows % (32 * PIECES) == 0
    chosen = dense_body if dense else slot_body
    return chosen(
        tokens, norm_gain, expert_ids, route_weight, gate_weight, up_weight, down_weight
    )


def solution(mesh):
    placed = (
        P(("grp", "ep"), None),
        P(),
        P(("grp", "ep"), None),
        P(("grp", "ep"), None),
        P("ep", None, None),
        P("ep", None, None),
        P("ep", None, None),
    )
    return jax.shard_map(
        body, mesh=mesh, in_specs=placed, out_specs=P(("grp", "ep"), None), check_vma=False
    )
```
